256 devices in a mesh: grp: 4 (over y, x), sp: 32 (over z), tp: 2 (over core).
Axes of the slice: x: 2, y: 2, z: 32, core: 2. Of those that a mesh axis runs over, the one named last changes fastest.
The devices are a block of a 4x8x32 slice.
Arguments:
- gate_in: bfloat16 [49152, 2048], P(('grp', 'sp'), 'tp'), parts along dimension 0, may hold values from -6 to 6
- values_in: bfloat16 [49152, 2048], P(('grp', 'sp'), 'tp'), parts along dimension 0, may hold values from -6 to 6
- input_state_in: bfloat16 [49152, 512], P(('grp', 'sp'), 'tp'), parts along dimension 0, may hold values from -6 to 6
- output_state_in: bfloat16 [49152, 512], P(('grp', 'sp'), 'tp'), parts along dimension 0, may hold values from -6 to 6
- step_in: bfloat16 [49152, 32], P(('grp', 'sp'), 'tp'), parts along dimension 0, may hold values from -6 to 6
- conv_x: bfloat16 [4, 2048], P(None, 'tp'), may hold values from -3 to 3
- conv_b: bfloat16 [4, 512], P(None, 'tp'), may hold values from -3 to 3
- conv_c: bfloat16 [4, 512], P(None, 'tp'), may hold values from -3 to 3
- dt_bias: float32 [32], P('tp'), may hold values from -1 to 1
- decay_rate: float32 [32], P('tp'), may hold values from 0 to 1, as said below
- log_decay_extra: float32 [49152, 32], P(('grp', 'sp'), 'tp'), parts along dimension 0, may hold values from -1 to 0
- out_gain: bfloat16 [2048], P('tp'), may hold values from 0.099609375 to 1.8984375
- w_out: bfloat16 [2048, 2048], P('tp'), may hold values from -0.125 to 0.125
Outputs:
- mixed: bfloat16 [49152, 2048], P(('grp', 'sp', 'tp')), parts along dimension 0
The draws below stay inside these ranges and needn't reach their ends.
There are 4 independent parts, one for each index of `grp`. The reference program is written for one: setup_inputs(seed, part) draws one part's arguments, and reference() takes and returns one part's arrays. A program takes and returns all parts, laid end to end along the dimension named above; an argument that names none is the same for every part. Nothing has to cross between parts.
Inputs may be any that keep to these rules, and one draw needn't show every extreme that they name: `decay_rate`: positive rates.
All inputs are finite; a program needn't handle non-finite values.
Results may differ from the reference program's by a relative error of at most 0.01.
Values may be sent and summed in bfloat16 or wider, within the bound.
No kernel may reach another device: no remote copies, remote signals or barrier semaphores. Data moves between devices by JAX's collectives and lax.ppermute only.
A program may use at most 128 MiB of HBM per device.

```python
import math
import jax
import jax.numpy as jnp
from jax import lax

D = 2048
MIXER_HEADS = 32
HEAD_DIM = 64
STATE = 128
GROUPS = 4
CONV = 4
BLOCK = 128
DEV_ROWS = 384
SEQUENCE_LENGTH = 12288
D_SSD = 2048


def draw_decay_rate(key, part):
    key_entries = jax.random.split(jax.random.fold_in(key, 11), 3)
    order = jax.random.permutation(key_entries[0], MIXER_HEADS)
    fast = order < MIXER_HEADS // 2
    slow_rate = jax.random.uniform(key_entries[1], (MIXER_HEADS,), jnp.float32, 0.3, 0.6) / SEQUENCE_LENGTH
    fast_rate = jnp.exp(jax.random.uniform(key_entries[2], (MIXER_HEADS,), jnp.float32, math.log(0.02), math.log(0.05)))
    return jnp.where(fast, fast_rate, slow_rate).astype(jnp.float32)


def draw_log_decay_extra(key, part):
    key_entries = jax.random.split(jax.random.fold_in(key, 23), 3)
    spans = SEQUENCE_LENGTH // DEV_ROWS
    factor = jnp.exp(jax.random.uniform(key_entries[0], (spans,), jnp.float32, math.log(0.1), math.log(1.5))) / SEQUENCE_LENGTH
    each_row_count = -jnp.repeat(factor, DEV_ROWS)
    group_token_rows = jax.random.randint(key_entries[1], (2,), 0, SEQUENCE_LENGTH)
    group_span_size = jax.random.uniform(key_entries[2], (2, MIXER_HEADS), jnp.float32, 0.2, 0.4)
    token_positions = jnp.arange(SEQUENCE_LENGTH)
    match_count = (token_positions[:, None] == group_token_rows[None, :]).astype(jnp.float32)
    token_groups = jnp.dot(match_count, jnp.log(1.0 - group_span_size), precision=jax.lax.Precision.HIGHEST)
    return (each_row_count[:, None] + token_groups).astype(jnp.float32)


def block_scale(stream_key, extent, cuts, low, high):
    level = 1.0
    for dim, parts in cuts:
        steps = jax.random.uniform(jax.random.fold_in(jax.random.fold_in(stream_key, 6), dim), (parts,), jnp.float32, low / len(cuts), high / len(cuts))
        level = level * jnp.repeat(jnp.exp(steps), extent[dim] // parts).reshape((-1,) + (1,) * (len(extent) - 1 - dim))
    return level


def centred(stream_key, extent, width, reach, cuts=(), kind=jnp.bfloat16):
    factor_of = block_scale(stream_key, extent, cuts, -0.22, 0.18) if cuts else 1.0
    drawn = jax.random.normal(stream_key, extent, jnp.float32) * width * factor_of
    return jnp.minimum(jnp.maximum(drawn, -reach), reach).astype(kind)


def setup_inputs(seed: int = 0, part: int = 0) -> dict:
    keys = jax.random.split(jax.random.key(seed), 14)
    part_splits = jax.random.split(jax.random.fold_in(keys[13], part), 14)
    return {
        "gate_in": centred(part_splits[0], (SEQUENCE_LENGTH, D_SSD), 1.0, 6.0, ((0, 32), (1, 2))),
        "values_in": centred(part_splits[1], (SEQUENCE_LENGTH, D_SSD), 1.0, 6.0, ((0, 32), (1, 2))),
        "input_state_in": centred(part_splits[2], (SEQUENCE_LENGTH, GROUPS * STATE), 1.0, 6.0, ((0, 32), (1, 2))),
        "output_state_in": centred(part_splits[3], (SEQUENCE_LENGTH, GROUPS * STATE), 1.0, 6.0, ((0, 32), (1, 2))),
        "step_in": centred(part_splits[4], (SEQUENCE_LENGTH, MIXER_HEADS), 1.0, 6.0, ((0, 32), (1, 2))),
        "conv_x": centred(keys[5], (CONV, D_SSD), CONV ** -0.5, 3.0, ((1, 2),)),
        "conv_b": centred(keys[6], (CONV, GROUPS * STATE), CONV ** -0.5, 3.0, ((1, 2),)),
        "conv_c": centred(keys[7], (CONV, GROUPS * STATE), CONV ** -0.5, 3.0, ((1, 2),)),
        "dt_bias": jnp.clip(jax.random.uniform(keys[8], (MIXER_HEADS,), jnp.float32, -1.0, 1.0) * block_scale(keys[8], (MIXER_HEADS,), ((0, 2),), -0.4, 0.0), -1.0, 1.0),
        "decay_rate": draw_decay_rate(jax.random.fold_in(keys[13], 71), part),
        "log_decay_extra": draw_log_decay_extra(jax.random.fold_in(jax.random.fold_in(keys[13], part), 71), part),
        "out_gain": jnp.clip(1.0 + 0.18 * jax.random.normal(keys[11], (D_SSD,), jnp.float32), 0.099609375, 1.8984375).astype(jnp.bfloat16),
        "w_out": centred(keys[12], (D_SSD, D), D_SSD ** -0.5, 0.125, ((0, 2),)),
    }


def rms_rows(values, gain, epsilon):
    floats = values.astype(jnp.float32)
    scaled = floats * lax.rsqrt(lax.optimization_barrier(jnp.mean(floats * floats, axis=-1, keepdims=True)) + epsilon)
    return scaled * gain.astype(jnp.float32)

def conv_silu(signal, kernel):
    length = signal.shape[0]
    padded = jnp.concatenate([jnp.zeros((CONV - 1, signal.shape[1]), jnp.bfloat16), signal], axis=0)
    summed = jnp.zeros(signal.shape, jnp.float32)
    for offset in range(CONV):
        summed = summed + kernel[offset].astype(jnp.float32) * padded[offset:offset + length].astype(jnp.float32)
    return jax.nn.silu(summed).astype(jnp.bfloat16)

def reference(gate_in, values_in, input_state_in, output_state_in, step_in, conv_x, conv_b, conv_c, dt_bias, decay_rate, log_decay_extra, out_gain, w_out):
    x_input = conv_silu(values_in, conv_x)
    b_input = conv_silu(input_state_in, conv_b)
    c_input = conv_silu(output_state_in, conv_c)
    step_size = jax.nn.softplus(step_in.astype(jnp.float32) + dt_bias.astype(jnp.float32))
    log_step = log_decay_extra.astype(jnp.float32) - step_size * decay_rate.astype(jnp.float32)
    per_group = MIXER_HEADS // GROUPS
    count = SEQUENCE_LENGTH // BLOCK
    lower = jnp.tril(jnp.ones((BLOCK, BLOCK), dtype=bool))

    def one_block(state, inputs):
        x_blk, b_blk, c_blk, step_blk, log_blk = inputs
        cum_log = jnp.cumsum(log_blk, axis=0)
        cum_rows = cum_log.T
        scores = jnp.einsum('ign,jgn->gij', c_blk.astype(jnp.float32), b_blk.astype(jnp.float32))
        head_scores = jnp.repeat(scores, per_group, axis=0)
        decay = jnp.exp(jnp.where(lower, cum_rows[:, :, None] - cum_rows[:, None, :], -jnp.inf))
        mixing = (head_scores * decay * step_blk.T[:, None, :]).astype(jnp.bfloat16)
        y_diag = jnp.einsum('hij,jhp->ihp', mixing.astype(jnp.float32), x_blk.astype(jnp.float32))
        to_end = jnp.exp(cum_rows[:, -1:] - cum_rows) * step_blk.T
        b_heads = (jnp.repeat(b_blk.astype(jnp.float32), per_group, axis=1) * to_end.T[:, :, None]).astype(jnp.bfloat16)
        added = jnp.einsum('jhp,jhn->hpn', x_blk.astype(jnp.float32), b_heads.astype(jnp.float32))
        c_heads = jnp.repeat(c_blk.astype(jnp.float32), per_group, axis=1)
        y_state = jnp.einsum('ihn,hpn->ihp', c_heads, state, precision=lax.Precision.HIGHEST) * jnp.exp(cum_log)[:, :, None]
        next_state = state * jnp.exp(cum_rows[:, -1])[:, None, None] + added
        return (next_state, y_diag + y_state)
    initial = jnp.zeros((MIXER_HEADS, HEAD_DIM, STATE), jnp.float32)
    inputs = (x_input.reshape(count, BLOCK, MIXER_HEADS, HEAD_DIM), b_input.reshape(count, BLOCK, GROUPS, STATE), c_input.reshape(count, BLOCK, GROUPS, STATE), step_size.reshape(count, BLOCK, MIXER_HEADS), log_step.reshape(count, BLOCK, MIXER_HEADS))
    _, outputs = lax.scan(one_block, initial, inputs)
    mixed_heads = outputs.reshape(SEQUENCE_LENGTH, MIXER_HEADS, HEAD_DIM)
    gated = mixed_heads * jax.nn.silu(gate_in.astype(jnp.float32)).reshape(SEQUENCE_LENGTH, MIXER_HEADS, HEAD_DIM)
    normalized = rms_rows(gated, out_gain.reshape(MIXER_HEADS, HEAD_DIM), 1e-05).astype(jnp.bfloat16).reshape(SEQUENCE_LENGTH, MIXER_HEADS * HEAD_DIM)
    return jnp.dot(normalized, w_out, preferred_element_type=jnp.float32).astype(jnp.bfloat16)
```

```python
import functools

import jax
import jax.numpy as jnp
from jax import lax
from jax.experimental import pallas as pl
from jax.experimental.pallas import tpu as pltpu
from jax.sharding import PartitionSpec as P

HEAD_DIM = 64
STATE = 128
CONV = 4
BLOCK = 128
QUAD = 4
EXTRA = 16
EPS = 1e-05
F32 = jnp.float32
BF16 = jnp.bfloat16
VMEM_LIMIT = 56 * 1024 * 1024


def dot(a, b, dims=((1,), (0,))):
    return lax.dot_general(a, b, (dims, ((), ())), preferred_element_type=F32)


def parts_of(x, count):
    out = []
    for _ in range(count):
        part = x.astype(BF16)
        out.append(part)
        x = x - part.astype(F32)
    return out


def spread_matrix(heads):
    row = lax.broadcasted_iota(jnp.int32, (heads, heads * HEAD_DIM), 0)
    col = lax.broadcasted_iota(jnp.int32, (heads, heads * HEAD_DIM), 1)
    return (row == col // HEAD_DIM).astype(F32).astype(BF16)


def spread(x, matrix, count=2):
    return sum(dot(part, matrix) for part in parts_of(x, count))


def softplus(x):
    return jnp.maximum(x, 0.0) + jnp.log1p(jnp.exp(-jnp.abs(x)))


def silu(x):
    return x / (1.0 + jnp.exp(-x))


def lower_ones(transposed=False):
    row = lax.broadcasted_iota(jnp.int32, (BLOCK, BLOCK), 0)
    col = lax.broadcasted_iota(jnp.int32, (BLOCK, BLOCK), 1)
    return (row <= col if transposed else row >= col).astype(F32).astype(BF16)


def block_cumsum(x, lower):
    heads = x.shape[1]
    summed = dot(lower, jnp.concatenate(parts_of(x, 3), axis=1))
    return summed[:, :heads] + summed[:, heads : 2 * heads] + summed[:, 2 * heads :]


def state_kernel(
    values, b_in, c_in, halo, step_in, extra, conv_x, conv_b, conv_c, dt_bias, rate,
    x_act, b_act, c_act, cum_out, step_out, slot0, slot1, slot2, slot3, ext, packed,
):
    span, inner = values.shape
    heads = step_in.shape[1]
    shared = b_in.shape[1]
    me = lax.rem(lax.axis_index("sp"), QUAD)
    step = softplus(step_in[...].astype(F32) + dt_bias[...])
    log_step = extra[...] - step * rate[...]
    step_out[...] = step
    lower = lower_ones()
    total = jnp.zeros((1, heads), F32)
    for block in range(span // BLOCK):
        rows = slice(block * BLOCK, (block + 1) * BLOCK)
        cum = block_cumsum(log_step[rows], lower) + total
        cum_out[rows, :] = cum
        total = cum[BLOCK - 1 :]
    weight = jnp.exp(total - cum_out[...]) * step
    matrix = spread_matrix(heads)
    width = 256
    offset = 0
    for source, taps, target in ((b_in, conv_b, b_act), (c_in, conv_c, c_act), (values, conv_x, x_act)):
        for start in range(0, source.shape[1], width):
            lanes = slice(start, start + width)
            position = offset + start
            ext[0:8, :] = halo[8:16, position : position + width].astype(F32)
            ext[8 : 8 + span, :] = source[:, lanes].astype(F32)
            summed = jnp.zeros((span, width), F32)
            for tap in range(CONV):
                summed = summed + taps[tap : tap + 1, lanes].astype(F32) * ext[8 - (CONV - 1) + tap : 8 - (CONV - 1) + tap + span, :]
            target[:, lanes] = silu(summed).astype(BF16)
        offset += source.shape[1]
    per_group = inner // (shared // STATE)
    for start in range(0, inner, width):
        lanes = slice(start, start + width)
        group = start // per_group
        weighted = (x_act[:, lanes].astype(F32) * spread(weight, matrix[:, lanes])).astype(BF16)
        state = dot(b_act[:, group * STATE : (group + 1) * STATE], weighted, ((0,), (0,)))
        packed[0:STATE, lanes] = state.astype(BF16)
    high, middle, low = (part.astype(F32) for part in parts_of(total, 3))
    row = lax.broadcasted_iota(jnp.int32, (EXTRA, heads), 0)
    logs = jnp.where(row == 0, high, jnp.where(row == 1, middle, jnp.where(row == 2, low, 0.0)))
    packed[STATE:, :] = dot(logs.astype(BF16), matrix).astype(BF16)
    quarter = inner // QUAD
    for bits, slot in enumerate((slot0, slot1, slot2, slot3)):
        slot[...] = packed[:, pl.ds(pl.multiple_of((me ^ bits) * quarter, 128), quarter)]


def whole(count):
    return [pl.BlockSpec(memory_space=pltpu.VMEM)] * count


def local_call(kernel, outs, args, scratch=(), flops=0, name=None):
    many = isinstance(outs, (list, tuple))
    size = sum(a.size * a.dtype.itemsize for a in args)
    return pl.pallas_call(
        kernel,
        out_shape=outs,
        in_specs=whole(len(args)),
        out_specs=whole(len(outs)) if many else whole(1)[0],
        scratch_shapes=list(scratch),
        compiler_params=pltpu.CompilerParams(vmem_limit_bytes=VMEM_LIMIT),
        cost_estimate=pl.CostEstimate(flops=flops, bytes_accessed=size, transcendentals=0),
        name=name,
    )(*args)


def load(ref):
    logs = ref[STATE:, :].astype(F32)
    return ref[0:STATE, :].astype(F32), logs[0:1] + logs[1:2] + logs[2:3]


def store(ref, state, log):
    ref[0:STATE, :] = state.astype(BF16)
    high, middle, low = (part.astype(F32) for part in parts_of(log, 3))
    row = lax.broadcasted_iota(jnp.int32, (EXTRA, log.shape[1]), 0)
    logs = jnp.where(row == 0, high, jnp.where(row == 1, middle, jnp.where(row == 2, low, 0.0)))
    ref[STATE:, :] = logs.astype(BF16)


def after(earlier, later):
    return earlier[0] * jnp.exp(later[1]) + later[0], earlier[1] + later[1]


def quad_order(ordered, refs):
    me = lax.rem(lax.axis_index("sp"), QUAD)
    for bits, ref in enumerate(refs):
        ordered[me ^ bits] = ref[...]


def quad_total_kernel(own, r1, r2, r3, out, ordered):
    quad_order(ordered, (own, r1, r2, r3))
    total = load(ordered.at[0])
    for place in range(1, QUAD):
        total = after(total, load(ordered.at[place]))
    store(out, *total)


def pair_kernel(distance, own, other, out):
    later = (lax.axis_index("sp") // distance) % 2 == 1

    @pl.when(later)
    def _():
        store(out, *after(load(other), load(own)))

    @pl.when(jnp.logical_not(later))
    def _():
        store(out, *after(load(own), load(other)))


def prefix_kernel(distances, *refs):
    count = len(distances)
    earlier, quad, outs, ordered, ends = refs[:count], refs[count : count + 4], refs[count + 4 : count + 8], refs[-2], refs[-1]
    place = lax.axis_index("sp")
    quad_order(ordered, quad)
    state = jnp.zeros((STATE, quad[0].shape[1]), F32)
    for distance, ref in zip(distances, earlier, strict=True):
        part, log = load(ref)
        later = (place // distance) % 2 == 1
        state = jnp.where(later, state * jnp.exp(log) + part, state)
    for turn in range(QUAD):
        ends[turn] = state.astype(BF16)
        if turn < QUAD - 1:
            part, log = load(ordered.at[turn])
            state = state * jnp.exp(log) + part
    me = lax.rem(place, QUAD)
    for bits, out in enumerate(outs):
        out[...] = ends[me ^ bits]


def inside_kernel(x_act, b_act, c_act, cum_all, step_all, y_out, padded, rows_cum, rows_step, entering):
    span, inner = x_act.shape
    heads = step_all.shape[1]
    groups = b_act.shape[1] // STATE
    per_group = heads // groups
    matrix = spread_matrix(heads)
    keep = lax.broadcasted_iota(jnp.int32, (BLOCK, BLOCK), 0) >= lax.broadcasted_iota(jnp.int32, (BLOCK, BLOCK), 1)
    left = lax.broadcasted_iota(jnp.int32, (BLOCK, 2 * HEAD_DIM), 1) < HEAD_DIM
    padded[...] = jnp.zeros_like(padded)
    before = jnp.zeros((1, heads), F32)
    for block in range(span // BLOCK):
        rows = slice(block * BLOCK, (block + 1) * BLOCK)
        cum = cum_all[rows, :] - before
        step = step_all[rows, :]
        padded[:, 0:heads] = cum
        rows_cum[...] = jnp.transpose(padded[...])
        padded[:, 0:heads] = step
        rows_step[...] = jnp.transpose(padded[...])
        total = cum[BLOCK - 1 :]
        before = before + total
        grow = jnp.exp(cum)
        weight = jnp.exp(total - cum) * step
        for group in range(groups):
            lanes = slice(group * STATE, (group + 1) * STATE)
            channels = slice(group * per_group * HEAD_DIM, (group + 1) * per_group * HEAD_DIM)
            b_blk, c_blk = b_act[rows, lanes], c_act[rows, lanes]
            scores = dot(c_blk, b_blk, ((1,), (1,)))
            for pair in range(per_group // 2):
                results = []
                for head in (group * per_group + 2 * pair, group * per_group + 2 * pair + 1):
                    difference = cum[:, head : head + 1] - rows_cum[head : head + 1, :]
                    decay = jnp.exp(jnp.where(keep, difference, -jnp.inf))
                    mixing = (scores * decay * rows_step[head : head + 1, :]).astype(BF16)
                    first = (group * per_group + 2 * pair) * HEAD_DIM
                    results.append(dot(mixing, x_act[rows, first : first + 2 * HEAD_DIM]))
                y_out[rows, first : first + 2 * HEAD_DIM] = jnp.where(left, results[0], results[1])
            if block > 0:
                read = dot(c_blk, entering[:, channels].astype(BF16))
                y_out[rows, channels] += read * spread(grow, matrix[:, channels])
            if block < span // BLOCK - 1:
                weighted = (x_act[rows, channels].astype(F32) * spread(weight, matrix[:, channels])).astype(BF16)
                added = dot(b_blk, weighted, ((0,), (0,)))
                if block > 0:
                    grown = spread(jnp.broadcast_to(jnp.exp(total), (8, heads)), matrix[:, channels], 3)[0:1]
                    added = entering[:, channels] * grown + added
                entering[:, channels] = added


def output_kernel(y_in, gate, c_act, cum_all, gain, p0, p1, p2, p3, out, ends):
    span, inner = y_in.shape
    heads = cum_all.shape[1]
    groups = c_act.shape[1] // STATE
    quarter = inner // QUAD
    matrix = spread_matrix(heads)
    me = lax.rem(lax.axis_index("sp"), QUAD)
    for bits, ref in enumerate((p0, p1, p2, p3)):
        ends[:, pl.ds(pl.multiple_of((me ^ bits) * quarter, 128), quarter)] = ref[...]
    same = lax.broadcasted_iota(jnp.int32, (quarter, quarter), 0) // HEAD_DIM == lax.broadcasted_iota(jnp.int32, (quarter, quarter), 1) // HEAD_DIM
    mean = (same.astype(F32) * (1.0 / HEAD_DIM)).astype(BF16)
    grow = jnp.exp(cum_all[...])
    for start in range(0, inner, quarter):
        lanes = slice(start, start + quarter)
        group = start // (inner // groups)
        read = dot(c_act[:, group * STATE : (group + 1) * STATE], ends[:, lanes])
        y = y_in[:, lanes] + read * spread(grow, matrix[:, lanes])
        gated = y * silu(gate[:, lanes].astype(F32))
        square = spread(gated * gated, mean)
        out[:, lanes] = (gated * lax.rsqrt(square + EPS) * gain[:, lanes].astype(F32)).astype(BF16)


def project_kernel(own, other, w_own, w_other, out):
    out[...] = (dot(own[...], w_own[...]) + dot(other[...], w_other[...])).astype(BF16)


def tail_kernel(values, b_in, c_in, out):
    inner, shared = values.shape[1], b_in.shape[1]
    out[:, 0:shared] = b_in[...]
    out[:, shared : 2 * shared] = c_in[...]
    out[:, 2 * shared : 2 * shared + inner] = values[...]


def body(
    gate_in, values_in, input_state_in, output_state_in, step_in, conv_x, conv_b, conv_c, dt_bias, decay_rate, log_decay_extra,
    out_gain, w_out,
):
    span, inner = values_in.shape
    shared = input_state_in.shape[1]
    heads = step_in.shape[1]
    places = lax.axis_size("sp")
    quarter = inner // QUAD
    shape = jax.ShapeDtypeStruct

    def move(x, route):
        return lax.ppermute(x, "sp", route)

    def exchange(x, bits):
        return move(x, [(i, i ^ bits) for i in range(places)])

    w_other = lax.ppermute(w_out, "tp", [(0, 1), (1, 0)])

    last = span // 16 - 1
    tail = pl.pallas_call(
        tail_kernel,
        out_shape=shape((16, inner + 2 * shared), BF16),
        grid=(1,),
        in_specs=[pl.BlockSpec((16, a.shape[1]), lambda i: (last, 0)) for a in (values_in, input_state_in, output_state_in)],
        out_specs=pl.BlockSpec((16, inner + 2 * shared), lambda i: (0, 0)),
        name="tail",
    )(values_in, input_state_in, output_state_in)
    halo = move(tail, [(i, i + 1) for i in range(places - 1)])

    payload = shape((STATE + EXTRA, quarter), BF16)
    x_act, b_act, c_act, cum, step, *slots = local_call(
        state_kernel,
        [
            shape((span, inner), BF16), shape((span, shared), BF16), shape((span, shared), BF16),
            shape((span, heads), F32), shape((span, heads), F32), payload, payload, payload, payload,
        ],
        [
            values_in, input_state_in, output_state_in, halo, step_in, log_decay_extra, conv_x, conv_b, conv_c,
            dt_bias.reshape(1, heads), decay_rate.reshape(1, heads),
        ],
        [pltpu.VMEM((span + 8, 256), F32), pltpu.VMEM((STATE + EXTRA, inner), BF16)],
        flops=2_000_000_000, name="state",
    )

    y_inside = local_call(
        inside_kernel,
        shape((span, inner), F32),
        [x_act, b_act, c_act, cum, step],
        [pltpu.VMEM((BLOCK, BLOCK), F32)] * 3 + [pltpu.VMEM((STATE, inner), F32)],
        flops=5_000_000_000, name="inside",
    )

    order = pltpu.VMEM((QUAD, STATE + EXTRA, quarter), BF16)
    arrived = {bits: exchange(slots[bits], bits) for bits in (3, 2, 1)}
    quad = [slots[0], arrived[1], arrived[2], arrived[3]]
    total = local_call(quad_total_kernel, payload, quad, [order], name="quad_total")
    distances, earlier = [], []
    distance = QUAD
    while distance < places // 2:
        other = exchange(total, distance)
        distances.insert(0, distance)
        earlier.insert(0, other)
        total = local_call(functools.partial(pair_kernel, distance), payload, [total, other], name="pair")
        distance *= 2
    fourth = places // 4
    route = [(i, (i + fourth) if i >= fourth else (i - fourth) % places) for i in range(places // 2)]
    distances.insert(0, distance)
    earlier.insert(0, move(total, route))
    ends = local_call(
        functools.partial(prefix_kernel, tuple(distances)),
        [shape((STATE, quarter), BF16)] * QUAD,
        [*earlier, *quad],
        [order, pltpu.VMEM((QUAD, STATE, quarter), BF16)],
        name="prefix",
    )
    carried = {bits: exchange(ends[bits], bits) for bits in (3, 2, 1)}
    normalized = local_call(
        output_kernel,
        shape((span, inner), BF16),
        [y_inside, gate_in, c_act, cum, out_gain.reshape(1, inner), ends[0], carried[1], carried[2], carried[3]],
        [pltpu.VMEM((STATE, inner), BF16)],
        name="output",
    )
    core = lax.axis_index("tp")
    half = span // 2
    mine = lax.dynamic_slice_in_dim(normalized, core * half, half, 0)
    theirs = lax.dynamic_slice_in_dim(normalized, (1 - core) * half, half, 0)
    other = lax.ppermute(theirs, "tp", [(0, 1), (1, 0)])
    return local_call(project_kernel, shape((half, w_out.shape[1]), BF16), [mine, other, w_out, w_other], name="project")


def solution(mesh):
    rows = P(("grp", "sp"), "tp")
    placed = (rows, rows, rows, rows, rows, P(None, "tp"), P(None, "tp"), P(None, "tp"), P("tp"), P("tp"), rows, P("tp"), P("tp", None))
    return jax.shard_map(body, mesh=mesh, in_specs=placed, out_specs=P(("grp", "sp", "tp"), None), check_vma=False)
```

```python
import functools

import jax
import jax.numpy as jnp
from jax import lax
from jax.experimental import pallas as pl
from jax.experimental.pallas import tpu as pltpu
from jax.sharding import PartitionSpec as P


HEAD_DIM = 64
STATE = 128
CONV = 4
BLOCK = 128
QUAD = 4
EXTRA = 16
EPS = 1e-05
F32 = jnp.float32
BF16 = jnp.bfloat16
EDGE = 16
FILL = 4_000_000_000
SMALL = 4 * 1024 * 1024
LARGE = 16 * 1024 * 1024
HUGE = 60 * 1024 * 1024


def dot(a, b, dims=((1,), (0,))):
    return lax.dot_general(a, b, (dims, ((), ())), preferred_element_type=F32)


def parts_of(x, count):
    out = []
    for _ in range(count):
        part = x.astype(BF16)
        out.append(part)
        x = x - part.astype(F32)
    return out


def spread_matrix(heads):
    row = lax.broadcasted_iota(jnp.int32, (heads, heads * HEAD_DIM), 0)
    col = lax.broadcasted_iota(jnp.int32, (heads, heads * HEAD_DIM), 1)
    return (row == col // HEAD_DIM).astype(F32).astype(BF16)


def spread(x, matrix, count=2):
    return dot(jnp.concatenate(parts_of(x, count), axis=0), jnp.concatenate([matrix] * count, axis=0), ((0,), (0,)))


def column(row):
    size = row.shape[1]
    same = lax.broadcasted_iota(jnp.int32, (size, size), 0) == lax.broadcasted_iota(jnp.int32, (size, size), 1)
    return jnp.sum(jnp.where(same, row, 0.0), axis=1, keepdims=True)


def softplus(x):
    return jnp.maximum(x, 0.0) + jnp.log1p(jnp.exp(-jnp.abs(x)))


def silu(x):
    return x / (1.0 + jnp.exp(-x))


def convolved(ext, first, rows, taps):
    summed = jnp.zeros((rows, ext.shape[1]), F32)
    for tap in range(CONV):
        summed = summed + taps[tap : tap + 1].astype(F32) * ext[first + tap : first + tap + rows, :]
    return silu(summed).astype(BF16)


def local_kernel(
    values, b_in, c_in, step_in, extra, conv_x, conv_b, conv_c, dt_bias, rate,
    x_act, b_act, c_act, cum_out, step_out, state_out, logs_out, edge_weight, ext,
):
    span, inner = values.shape
    heads = step_in.shape[0]
    step = softplus(step_in[...].astype(F32) + column(dt_bias[...]))
    log_step = extra[...] - step * column(rate[...])
    step_out[...] = step
    row = lax.broadcasted_iota(jnp.int32, (BLOCK, BLOCK), 0)
    upper = (row <= lax.broadcasted_iota(jnp.int32, (BLOCK, BLOCK), 1)).astype(F32).astype(BF16)
    total = jnp.zeros((heads, 1), F32)
    for start in range(0, span, BLOCK):
        summed = dot(jnp.concatenate(parts_of(log_step[:, start : start + BLOCK], 3), axis=0), upper)
        cum = summed[:heads] + summed[heads : 2 * heads] + summed[2 * heads :] + total
        cum_out[:, start : start + BLOCK] = cum
        total = cum[:, BLOCK - 1 :]
    matrix = spread_matrix(heads)
    weight = jnp.exp(total - cum_out[...]) * step
    edge_weight[...] = spread(weight[:, 0:BLOCK], matrix)[0:EDGE]
    lane = lax.broadcasted_iota(jnp.int32, (heads, BLOCK), 1)
    high, middle, low = (part.astype(F32) for part in parts_of(total, 3))
    logs = jnp.where(lane == 0, high, jnp.where(lane == 1, middle, jnp.where(lane == 2, low, 0.0)))
    logs_out[...] = dot(logs.astype(BF16), matrix, ((0,), (0,)))[0:EXTRA].astype(BF16)
    weight = jnp.where(lax.broadcasted_iota(jnp.int32, (heads, span), 1) < EDGE, 0.0, weight)
    width = ext.shape[1]
    ext[0:8, :] = jnp.zeros((8, width), F32)
    per_group = inner // (b_in.shape[1] // STATE)
    for source, taps, target in ((b_in, conv_b, b_act), (c_in, conv_c, c_act), (values, conv_x, x_act)):
        for start in range(0, source.shape[1], width):
            lanes = slice(start, start + width)
            ext[8 : 8 + span, :] = source[:, lanes].astype(F32)
            active = convolved(ext, 8 - (CONV - 1), span, taps[:, lanes])
            target[:, lanes] = active
            if source is values:
                group = start // per_group
                weighted = (active.astype(F32) * spread(weight, matrix[:, lanes])).astype(BF16)
                state_out[:, lanes] = dot(b_act[:, group * STATE : (group + 1) * STATE], weighted, ((0,), (0,)))


def edge_kernel(
    values, b_in, c_in, halo, conv_x, conv_b, conv_c, state_in, logs_in, edge_weight,
    edge_x, edge_b, edge_c, slot0, slot1, slot2, slot3, ext, packed,
):
    inner, shared = values.shape[1], b_in.shape[1]
    offset = 0
    for source, taps, target in ((b_in, conv_b, edge_b), (c_in, conv_c, edge_c), (values, conv_x, edge_x)):
        lanes = slice(offset, offset + source.shape[1])
        part = ext.at[:, lanes]
        part[0:EDGE, :] = halo[:, lanes].astype(F32)
        part[EDGE : 2 * EDGE, :] = source[...].astype(F32)
        target[...] = convolved(part, EDGE - (CONV - 1), EDGE, taps[...])
        offset += source.shape[1]
    groups = shared // STATE
    weighted = (edge_x[...].astype(F32) * edge_weight[...]).astype(BF16)
    for group in range(groups):
        lanes = slice(group * (inner // groups), (group + 1) * (inner // groups))
        added = dot(edge_b[:, group * STATE : (group + 1) * STATE], weighted[:, lanes], ((0,), (0,)))
        packed[0:STATE, lanes] = (state_in[:, lanes] + added).astype(BF16)
    packed[STATE:, :] = logs_in[...]
    me = lax.rem(lax.axis_index("sp"), QUAD)
    quarter = inner // QUAD
    for bits, slot in enumerate((slot0, slot1, slot2, slot3)):
        slot[...] = packed[:, pl.ds(pl.multiple_of((me ^ bits) * quarter, 128), quarter)]


def whole(count):
    return [pl.BlockSpec(memory_space=pltpu.VMEM)] * count


def local_call(kernel, outs, args, scratch=(), flops=0, limit=None):
    many = isinstance(outs, (list, tuple))
    size = sum(a.size * a.dtype.itemsize for a in args)
    return pl.pallas_call(
        kernel,
        out_shape=outs,
        in_specs=whole(len(args)),
        out_specs=whole(len(outs)) if many else whole(1)[0],
        scratch_shapes=list(scratch),
        compiler_params=pltpu.CompilerParams(vmem_limit_bytes=limit or LARGE),
        cost_estimate=pl.CostEstimate(flops=flops, bytes_accessed=size, transcendentals=0),
    )(*args)


def load(ref):
    logs = ref[STATE:, :].astype(F32)
    return ref[0:STATE, :].astype(F32), logs[0:1] + logs[1:2] + logs[2:3]


def store(ref, state, log):
    ref[0:STATE, :] = state.astype(BF16)
    high, middle, low = (part.astype(F32) for part in parts_of(log, 3))
    row = lax.broadcasted_iota(jnp.int32, (EXTRA, log.shape[1]), 0)
    logs = jnp.where(row == 0, high, jnp.where(row == 1, middle, jnp.where(row == 2, low, 0.0)))
    ref[STATE:, :] = logs.astype(BF16)


def after(earlier, later):
    return earlier[0] * jnp.exp(later[1]) + later[0], earlier[1] + later[1]


def quad_order(ordered, refs):
    me = lax.rem(lax.axis_index("sp"), QUAD)
    for bits, ref in enumerate(refs):
        ordered[me ^ bits] = ref[...]


def quad_total_kernel(own, r1, r2, r3, out, ordered):
    quad_order(ordered, (own, r1, r2, r3))
    total = load(ordered.at[0])
    for place in range(1, QUAD):
        total = after(total, load(ordered.at[place]))
    store(out, *total)


def pair_kernel(distance, own, other, out):
    later = (lax.axis_index("sp") // distance) % 2 == 1

    @pl.when(later)
    def _():
        store(out, *after(load(other), load(own)))

    @pl.when(jnp.logical_not(later))
    def _():
        store(out, *after(load(own), load(other)))


def prefix_kernel(distances, top, low, up, *refs):
    count = len(distances) - 1
    earlier, quad, outs, ordered, ends = refs[:count], refs[count : count + 4], refs[count + 4 : count + 8], refs[-2], refs[-1]
    place = lax.axis_index("sp")
    quad_order(ordered, quad)
    state = top[0:STATE, :].astype(F32)
    for distance, ref in zip((*distances[:1], *distances), (up, low, *earlier), strict=True):
        part, log = load(ref)
        later = (place // distance) % 2 == 1
        state = jnp.where(later, state * jnp.exp(log) + part, state)
    for turn in range(QUAD):
        ends[turn] = state.astype(BF16)
        if turn < QUAD - 1:
            part, log = load(ordered.at[turn])
            state = state * jnp.exp(log) + part
    me = lax.rem(place, QUAD)
    for bits, out in enumerate(outs):
        out[...] = ends[me ^ bits]


def gate_kernel(gate, cum_all, gate_out, grow_out):
    matrix = spread_matrix(cum_all.shape[0])
    width = 256
    grow = jnp.exp(cum_all[...])
    for start in range(0, gate.shape[1], width):
        lanes = slice(start, start + width)
        gated = silu(gate[:, lanes].astype(F32))
        gate_out[:, lanes] = gated
        grow_out[:, lanes] = gated * spread(grow, matrix[:, lanes])


def inside_kernel(
    x_act, b_act, c_act, edge_x, edge_b, edge_c, cum_all, step_all, gate,
    y_out, c_out, b_all, x_first, padded, turned, entering,
):
    span, _ = x_act.shape
    heads = step_all.shape[0]
    groups = b_act.shape[1] // STATE
    per_group = heads // groups
    matrix = spread_matrix(heads)
    keep = lax.broadcasted_iota(jnp.int32, (BLOCK, BLOCK), 0) >= lax.broadcasted_iota(jnp.int32, (BLOCK, BLOCK), 1)
    left = lax.broadcasted_iota(jnp.int32, (BLOCK, 2 * HEAD_DIM), 1) < HEAD_DIM
    c_out[...] = c_act[...]
    c_out[0:EDGE, :] = edge_c[...]
    b_all[...] = b_act[...]
    b_all[0:EDGE, :] = edge_b[...]
    x_first[...] = x_act[0:BLOCK, :]
    x_first[0:EDGE, :] = edge_x[...]
    padded[...] = jnp.zeros_like(padded)
    before = jnp.zeros((heads, 1), F32)
    for start in range(0, span, BLOCK):
        rows = slice(start, start + BLOCK)
        x_blk = x_first if start == 0 else x_act.at[rows]
        cum = cum_all[:, rows] - before
        step = step_all[:, rows]
        padded[0:heads, :] = cum
        turned[...] = jnp.transpose(padded[...])
        total = cum[:, BLOCK - 1 :]
        before = before + total
        grow = jnp.exp(cum)
        weight = jnp.exp(total - cum) * step
        for group in range(groups):
            lanes = slice(group * STATE, (group + 1) * STATE)
            channels = slice(group * per_group * HEAD_DIM, (group + 1) * per_group * HEAD_DIM)
            b_blk, c_blk = b_all[rows, lanes], c_out[rows, lanes]
            scores = dot(c_blk, b_blk, ((1,), (1,)))
            if start > 0:
                read = dot(c_blk, entering[:, channels].astype(BF16)) * spread(grow, matrix[:, channels])
            for pair in range(per_group // 2):
                first = (group * per_group + 2 * pair) * HEAD_DIM
                results = []
                for head in (group * per_group + 2 * pair, group * per_group + 2 * pair + 1):
                    difference = turned[:, head : head + 1] - cum[head : head + 1, :]
                    decay = jnp.exp(jnp.where(keep, difference, -jnp.inf))
                    mixing = (scores * decay * step[head : head + 1, :]).astype(BF16)
                    results.append(dot(mixing, x_blk[:, first : first + 2 * HEAD_DIM]))
                y = jnp.where(left, results[0], results[1])
                if start > 0:
                    y = y + read[:, 2 * pair * HEAD_DIM : 2 * (pair + 1) * HEAD_DIM]
                y_out[rows, first : first + 2 * HEAD_DIM] = y * gate[rows, first : first + 2 * HEAD_DIM]
            if start + BLOCK < span:
                weighted = (x_blk[:, channels].astype(F32) * spread(weight, matrix[:, channels])).astype(BF16)
                added = dot(b_blk, weighted, ((0,), (0,)))
                if start > 0:
                    grown = spread(jnp.broadcast_to(jnp.exp(total), (heads, BLOCK)), matrix[:, channels], 3)
                    added = entering[:, channels] * grown + added
                entering[:, channels] = added


def output_kernel(own, y_in, grow, c_all, gain, p0, p1, p2, p3, out, ends):
    span, inner = y_in.shape
    groups = c_all.shape[1] // STATE
    quarter = inner // QUAD
    half = span // 2
    core = lax.axis_index("tp")
    rows = pl.ds(pl.multiple_of((core if own else 1 - core) * half, 64), half)
    me = lax.rem(lax.axis_index("sp"), QUAD)
    for bits, ref in enumerate((p0, p1, p2, p3)):
        ends[:, pl.ds(pl.multiple_of((me ^ bits) * quarter, 128), quarter)] = ref[...]
    place = lax.broadcasted_iota(jnp.int32, (quarter, quarter), 0) // HEAD_DIM
    same = place == lax.broadcasted_iota(jnp.int32, (quarter, quarter), 1) // HEAD_DIM
    mean = (same.astype(F32) * (1.0 / HEAD_DIM)).astype(BF16)
    for start in range(0, inner, quarter):
        lanes = slice(start, start + quarter)
        group = start // (inner // groups)
        read = dot(c_all[rows, group * STATE : (group + 1) * STATE], ends[:, lanes])
        gated = y_in[rows, lanes] + read * grow[rows, lanes]
        square = sum(dot(part, mean) for part in parts_of(gated * gated, 2))
        out[:, lanes] = (gated * lax.rsqrt(square + EPS) * gain[:, lanes].astype(F32)).astype(BF16)


def own_kernel(mine, w_own, out):
    out[...] = dot(mine[...], w_own[...])


def sum_kernel(own, other, w_other, out):
    out[...] = (own[...] + dot(other[...], w_other[...])).astype(BF16)


def tail_kernel(values, b_in, c_in, out, sems):
    offset, copies = 0, []
    for turn, source in enumerate((b_in, c_in, values)):
        rows, lanes = pl.ds(source.shape[0] - EDGE, EDGE), pl.ds(offset, source.shape[1])
        copies.append(pltpu.make_async_copy(source.at[rows, :], out.at[:, lanes], sems.at[turn]))
        offset += source.shape[1]
    for copy in copies:
        copy.start()
    for copy in copies:
        copy.wait()


def body(
    gate_in, values_in, input_state_in, output_state_in, step_in, conv_x, conv_b, conv_c, dt_bias, decay_rate, log_decay_extra,
    out_gain, w_out,
):
    span, inner = values_in.shape
    shared = input_state_in.shape[1]
    heads = step_in.shape[1]
    places = lax.axis_size("sp")
    quarter = inner // QUAD
    shape = jax.ShapeDtypeStruct
    vmem = pltpu.VMEM

    def move(x, route):
        return lax.ppermute(x, "sp", route)

    def exchange(x, bits, count=places):
        return move(x, [(i, i ^ bits) for i in range(count)])

    def edge_specs(block):
        return [pl.BlockSpec((EDGE, a.shape[1]), lambda i: (block, 0)) for a in (values_in, input_state_in, output_state_in)]

    tail = pl.pallas_call(
        tail_kernel,
        out_shape=shape((EDGE, inner + 2 * shared), BF16),
        in_specs=[pl.BlockSpec(memory_space=pl.ANY)] * 3,
        out_specs=whole(1)[0],
        scratch_shapes=[pltpu.SemaphoreType.DMA((3,))],
        compiler_params=pltpu.CompilerParams(vmem_limit_bytes=HUGE),
        name="tail",
    )(values_in, input_state_in, output_state_in)
    halo = move(tail, [(i, i + 1) for i in range(places - 1)])

    x_act, b_act, c_act, cum, step, state, logs, edge_weight = local_call(
        local_kernel,
        [
            shape((span, inner), BF16), shape((span, shared), BF16), shape((span, shared), BF16), shape((heads, span), F32),
            shape((heads, span), F32), shape((STATE, inner), F32), shape((EXTRA, inner), BF16), shape((EDGE, inner), F32),
        ],
        [
            values_in, input_state_in, output_state_in, step_in.T, log_decay_extra.T, conv_x, conv_b, conv_c,
            dt_bias.reshape(1, heads), decay_rate.reshape(1, heads),
        ],
        [vmem((span + 8, 256), F32)],
        flops=FILL,
    )
    payload = shape((STATE + EXTRA, quarter), BF16)
    edge_x, edge_b, edge_c, *slots = pl.pallas_call(
        edge_kernel,
        out_shape=[
            shape((EDGE, inner), BF16), shape((EDGE, shared), BF16), shape((EDGE, shared), BF16), payload, payload, payload, payload,
        ],
        grid=(1,),
        in_specs=edge_specs(0) + whole(7),
        out_specs=whole(7),
        scratch_shapes=[vmem((2 * EDGE, inner + 2 * shared), F32), vmem((STATE + EXTRA, inner), BF16)],
        compiler_params=pltpu.CompilerParams(vmem_limit_bytes=SMALL),
        name="edge",
    )(values_in, input_state_in, output_state_in, halo, conv_x, conv_b, conv_c, state, logs, edge_weight)
    gate, grow = local_call(gate_kernel, [shape((span, inner), F32)] * 2, [gate_in, cum], flops=FILL)
    y_inside, c_all = local_call(
        inside_kernel,
        [shape((span, inner), F32), shape((span, shared), BF16)],
        [x_act, b_act, c_act, edge_x, edge_b, edge_c, cum, step, gate],
        [
            vmem((span, shared), BF16), vmem((BLOCK, inner), BF16), vmem((BLOCK, BLOCK), F32), vmem((BLOCK, BLOCK), F32),
            vmem((STATE, inner), F32),
        ],
        flops=FILL,
    )

    order = vmem((QUAD, STATE + EXTRA, quarter), BF16)
    arrived = {bits: exchange(slots[bits], bits) for bits in (3, 2, 1)}
    quad = [slots[0], arrived[1], arrived[2], arrived[3]]
    total = local_call(quad_total_kernel, payload, quad, [order], limit=SMALL)
    distances, earlier = [], []
    distance = QUAD
    while distance < places // 4:
        other = exchange(total, distance)
        distances.insert(0, distance)
        earlier.insert(0, other)
        total = local_call(functools.partial(pair_kernel, distance), payload, [total, other], limit=SMALL)
        distance *= 2
    other = exchange(total, distance, places // 2)
    upper = move(total, [(i, i + distance) for i in range(places // 2, places - distance)])
    distances.insert(0, distance)
    total = local_call(functools.partial(pair_kernel, distance), payload, [total, other], limit=SMALL)
    route = [(i, (i + distance) if i >= distance else (i - distance) % places) for i in range(places // 2)]
    top = move(total, route)
    w_other, _ = lax.optimization_barrier((w_out, total))
    w_other = lax.ppermute(w_other, "tp", [(0, 1), (1, 0)])
    ends = local_call(
        functools.partial(prefix_kernel, tuple(distances)),
        [shape((STATE, quarter), BF16)] * QUAD,
        [top, other, upper, *earlier, *quad],
        [order, vmem((QUAD, STATE, quarter), BF16)],
        limit=SMALL,
    )
    carried = {bits: exchange(ends[bits], bits) for bits in (3, 2, 1)}

    def normalized(own):
        return local_call(
            functools.partial(output_kernel, own),
            shape((span // 2, inner), BF16),
            [y_inside, grow, c_all, out_gain.reshape(1, inner), ends[0], carried[1], carried[2], carried[3]],
            [vmem((STATE, inner), BF16)],
        )

    theirs = normalized(False)
    other_rows = lax.ppermute(theirs, "tp", [(0, 1), (1, 0)])
    mine = normalized(True)
    wide = shape((span // 2, w_out.shape[1]), F32)
    own = local_call(own_kernel, wide, [mine, w_out], flops=FILL)
    return local_call(sum_kernel, shape(wide.shape, BF16), [own, other_rows, w_other])


def solution(mesh):
    rows = P(("grp", "sp"), "tp")
    placed = (rows, rows, rows, rows, rows, P(None, "tp"), P(None, "tp"), P(None, "tp"), P("tp"), P("tp"), rows, P("tp"), P("tp", None))
    return jax.shard_map(body, mesh=mesh, in_specs=placed, out_specs=P(("grp", "sp", "tp"), None), check_vma=False)
```

```python
import functools

import jax
import jax.numpy as jnp
from jax import lax
from jax.experimental import pallas as pl
from jax.experimental.pallas import tpu as pltpu
from jax.sharding import PartitionSpec as P


HEAD_DIM = 64
STATE = 128
CONV = 4
BLOCK = 128
QUAD = 4
EXTRA = 16
EPS = 1e-05
F32 = jnp.float32
BF16 = jnp.bfloat16
EDGE = 16
FILL = 4_000_000_000
SMALL = 4 * 1024 * 1024
LARGE = 16 * 1024 * 1024


def dot(a, b, dims=((1,), (0,))):
    return lax.dot_general(a, b, (dims, ((), ())), preferred_element_type=F32)


def parts_of(x, count):
    out = []
    for _ in range(count):
        part = x.astype(BF16)
        out.append(part)
        x = x - part.astype(F32)
    return out


def spread_matrix(heads):
    row = lax.broadcasted_iota(jnp.int32, (heads, heads * HEAD_DIM), 0)
    col = lax.broadcasted_iota(jnp.int32, (heads, heads * HEAD_DIM), 1)
    return (row == col // HEAD_DIM).astype(F32).astype(BF16)


def spread(x, matrix, count=2):
    return dot(jnp.concatenate(parts_of(x, count), axis=0), jnp.concatenate([matrix] * count, axis=0), ((0,), (0,)))


def column(row):
    size = row.shape[1]
    same = lax.broadcasted_iota(jnp.int32, (size, size), 0) == lax.broadcasted_iota(jnp.int32, (size, size), 1)
    return jnp.sum(jnp.where(same, row, 0.0), axis=1, keepdims=True)


def softplus(x):
    return jnp.maximum(x, 0.0) + jnp.log1p(jnp.exp(-jnp.abs(x)))


def silu(x):
    return x / (1.0 + jnp.exp(-x))


def convolved(ext, first, rows, taps):
    summed = jnp.zeros((rows, ext.shape[1]), F32)
    for tap in range(CONV):
        summed = summed + taps[tap : tap + 1].astype(F32) * ext[first + tap : first + tap + rows, :]
    return silu(summed).astype(BF16)


def local_kernel(
    values_hbm, b_hbm, c_hbm, step_hbm, extra_hbm, conv_x_hbm, conv_b_hbm, conv_c_hbm, dt_hbm, rate_hbm,
    x_act, b_act, c_act, cum_out, step_out, state_out, logs_out, edge_weight,
    ext, values, b_in, c_in, step_in, extra, conv_x, conv_b, conv_c, dt_bias, rate, sems,
):
    sources = (step_hbm, extra_hbm, dt_hbm, rate_hbm, b_hbm, conv_b_hbm, c_hbm, conv_c_hbm, values_hbm, conv_x_hbm)
    targets = (step_in, extra, dt_bias, rate, b_in, conv_b, c_in, conv_c, values, conv_x)
    copies = [pltpu.make_async_copy(source, target, sems.at[turn]) for turn, (source, target) in enumerate(zip(sources, targets, strict=True))]
    for copy in copies:
        copy.start()
    for copy in copies[:4]:
        copy.wait()
    span, inner = values.shape
    heads = step_in.shape[0]
    step = softplus(step_in[...].astype(F32) + column(dt_bias[...]))
    log_step = extra[...] - step * column(rate[...])
    step_out[...] = step
    row = lax.broadcasted_iota(jnp.int32, (BLOCK, BLOCK), 0)
    upper = (row <= lax.broadcasted_iota(jnp.int32, (BLOCK, BLOCK), 1)).astype(F32).astype(BF16)
    total = jnp.zeros((heads, 1), F32)
    for start in range(0, span, BLOCK):
        summed = dot(jnp.concatenate(parts_of(log_step[:, start : start + BLOCK], 3), axis=0), upper)
        cum = summed[:heads] + summed[heads : 2 * heads] + summed[2 * heads :] + total
        cum_out[:, start : start + BLOCK] = cum
        total = cum[:, BLOCK - 1 :]
    matrix = spread_matrix(heads)
    weight = jnp.exp(total - cum_out[...]) * step
    edge_weight[...] = spread(weight[:, 0:BLOCK], matrix)[0:EDGE]
    lane = lax.broadcasted_iota(jnp.int32, (heads, BLOCK), 1)
    high, middle, low = (part.astype(F32) for part in parts_of(total, 3))
    logs = jnp.where(lane == 0, high, jnp.where(lane == 1, middle, jnp.where(lane == 2, low, 0.0)))
    logs_out[...] = dot(logs.astype(BF16), matrix, ((0,), (0,)))[0:EXTRA].astype(BF16)
    weight = jnp.where(lax.broadcasted_iota(jnp.int32, (heads, span), 1) < EDGE, 0.0, weight)
    width = ext.shape[1]
    ext[0:8, :] = jnp.zeros((8, width), F32)
    per_group = inner // (b_in.shape[1] // STATE)
    for turn, (source, taps, target) in enumerate(((b_in, conv_b, b_act), (c_in, conv_c, c_act), (values, conv_x, x_act))):
        for copy in copies[4 + 2 * turn : 6 + 2 * turn]:
            copy.wait()
        for start in range(0, source.shape[1], width):
            lanes = slice(start, start + width)
            ext[8 : 8 + span, :] = source[:, lanes].astype(F32)
            active = convolved(ext, 8 - (CONV - 1), span, taps[:, lanes])
            target[:, lanes] = active
            if source is values:
                group = start // per_group
                weighted = (active.astype(F32) * spread(weight, matrix[:, lanes])).astype(BF16)
                state_out[:, lanes] = dot(b_act[:, group * STATE : (group + 1) * STATE], weighted, ((0,), (0,)))


def edge_kernel(
    values, b_in, c_in, halo, conv_x, conv_b, conv_c, state_in, logs_in, edge_weight,
    edge_x, edge_b, edge_c, slot0, slot1, slot2, slot3, ext, packed,
):
    inner, shared = values.shape[1], b_in.shape[1]
    offset = 0
    for source, taps, target in ((b_in, conv_b, edge_b), (c_in, conv_c, edge_c), (values, conv_x, edge_x)):
        lanes = slice(offset, offset + source.shape[1])
        part = ext.at[:, lanes]
        part[0:EDGE, :] = halo[:, lanes].astype(F32)
        part[EDGE : 2 * EDGE, :] = source[...].astype(F32)
        target[...] = convolved(part, EDGE - (CONV - 1), EDGE, taps[...])
        offset += source.shape[1]
    groups = shared // STATE
    weighted = (edge_x[...].astype(F32) * edge_weight[...]).astype(BF16)
    for group in range(groups):
        lanes = slice(group * (inner // groups), (group + 1) * (inner // groups))
        added = dot(edge_b[:, group * STATE : (group + 1) * STATE], weighted[:, lanes], ((0,), (0,)))
        packed[0:STATE, lanes] = (state_in[:, lanes] + added).astype(BF16)
    packed[STATE:, :] = logs_in[...]
    me = lax.rem(lax.axis_index("sp"), QUAD)
    quarter = inner // QUAD
    for bits, slot in enumerate((slot0, slot1, slot2, slot3)):
        slot[...] = packed[:, pl.ds(pl.multiple_of((me ^ bits) * quarter, 128), quarter)]


def whole(count):
    return [pl.BlockSpec(memory_space=pltpu.VMEM)] * count


def local_call(kernel, outs, args, scratch=(), flops=0, limit=None):
    many = isinstance(outs, (list, tuple))
    size = sum(a.size * a.dtype.itemsize for a in args)
    return pl.pallas_call(
        kernel,
        out_shape=outs,
        in_specs=whole(len(args)),
        out_specs=whole(len(outs)) if many else whole(1)[0],
        scratch_shapes=list(scratch),
        compiler_params=pltpu.CompilerParams(vmem_limit_bytes=limit or LARGE),
        cost_estimate=pl.CostEstimate(flops=flops, bytes_accessed=size, transcendentals=0),
    )(*args)


def load(ref):
    logs = ref[STATE:, :].astype(F32)
    return ref[0:STATE, :].astype(F32), logs[0:1] + logs[1:2] + logs[2:3]


def quad_order(ordered, refs):
    me = lax.rem(lax.axis_index("sp"), QUAD)
    for bits, ref in enumerate(refs):
        ordered[me ^ bits] = ref[...]


def store(ref, state, log):
    ref[0:STATE, :] = state.astype(BF16)
    high, middle, low = (part.astype(F32) for part in parts_of(log, 3))
    row = lax.broadcasted_iota(jnp.int32, (EXTRA, log.shape[1]), 0)
    logs = jnp.where(row == 0, high, jnp.where(row == 1, middle, jnp.where(row == 2, low, 0.0)))
    ref[STATE:, :] = logs.astype(BF16)


def quad_total_kernel(own, r1, r2, r3, sent, state_out, log_out, ordered):
    quad_order(ordered, (own, r1, r2, r3))
    state, log = load(ordered.at[0])
    for place in range(1, QUAD):
        part, part_log = load(ordered.at[place])
        state, log = state * jnp.exp(part_log) + part, log + part_log
    store(sent, state, log)
    state_out[...] = state
    log_out[...] = log


def hop_kernel(half, turn, before, total, total_log, out):
    @pl.when(lax.rem(lax.axis_index("sp") // QUAD, half) == turn)
    def _():
        state, log = load(before)
        store(out, state * jnp.exp(total_log[...]) + total[...], log + total_log[...])


def top_kernel(half, before, total, total_log, out):
    @pl.when(lax.axis_index("sp") // QUAD == half - 1)
    def _():
        out[...] = (before[0:STATE, :].astype(F32) * jnp.exp(total_log[...]) + total[...]).astype(BF16)


def relay_kernel(half, own, got, out):
    @pl.when(lax.axis_index("sp") // QUAD == half - 1)
    def _():
        out[...] = own[...]

    @pl.when(lax.axis_index("sp") // QUAD == half + 1)
    def _():
        out[...] = got[...]


def prefix_kernel(half, *refs):
    passed, tops, quad, outs = refs[: half - 1], refs[half - 1 : half + 2], refs[half + 2 : half + 6], refs[half + 6 : half + 10]
    ordered, ends, held, top = refs[half + 10 :]
    place = lax.axis_index("sp")
    group = place // QUAD
    quad_order(ordered, quad)
    held[...] = jnp.zeros_like(held)
    top[...] = jnp.zeros_like(top)
    for turn, ref in enumerate(passed):

        @pl.when(lax.rem(group, half) == turn + 1)
        def _(ref=ref):
            held[...] = ref[...]

    for ref, targets in zip(tops, ((half + 1,), (half + 3,), (half, half + 2)), strict=True):
        for target in targets:

            @pl.when(group == target)
            def _(ref=ref):
                top[...] = ref[...]

    state, log = load(held)
    state = top[...].astype(F32) * jnp.exp(log) + state
    ends[0] = state.astype(BF16)
    for turn in range(QUAD - 1):
        part, log = load(ordered.at[turn])
        state = state * jnp.exp(log) + part
        ends[turn + 1] = state.astype(BF16)
    me = lax.rem(place, QUAD)
    for bits, out in enumerate(outs):
        out[...] = ends[me ^ bits]


def gate_kernel(gate, cum_all, gate_out, grow_out):
    matrix = spread_matrix(cum_all.shape[0])
    width = 256
    grow = jnp.exp(cum_all[...])
    for start in range(0, gate.shape[1], width):
        lanes = slice(start, start + width)
        gated = silu(gate[:, lanes].astype(F32))
        gate_out[:, lanes] = gated
        grow_out[:, lanes] = gated * spread(grow, matrix[:, lanes])


def inside_kernel(
    x_act, b_act, c_act, edge_x, edge_b, edge_c, cum_all, step_all, gate,
    y_out, c_out, b_all, x_first, padded, turned, entering,
):
    span, _ = x_act.shape
    heads = step_all.shape[0]
    groups = b_act.shape[1] // STATE
    per_group = heads // groups
    matrix = spread_matrix(heads)
    keep = lax.broadcasted_iota(jnp.int32, (BLOCK, BLOCK), 0) >= lax.broadcasted_iota(jnp.int32, (BLOCK, BLOCK), 1)
    left = lax.broadcasted_iota(jnp.int32, (BLOCK, 2 * HEAD_DIM), 1) < HEAD_DIM
    c_out[...] = c_act[...]
    c_out[0:EDGE, :] = edge_c[...]
    b_all[...] = b_act[...]
    b_all[0:EDGE, :] = edge_b[...]
    x_first[...] = x_act[0:BLOCK, :]
    x_first[0:EDGE, :] = edge_x[...]
    padded[...] = jnp.zeros_like(padded)
    before = jnp.zeros((heads, 1), F32)
    for start in range(0, span, BLOCK):
        rows = slice(start, start + BLOCK)
        x_blk = x_first if start == 0 else x_act.at[rows]
        cum = cum_all[:, rows] - before
        step = step_all[:, rows]
        padded[0:heads, :] = cum
        turned[...] = jnp.transpose(padded[...])
        total = cum[:, BLOCK - 1 :]
        before = before + total
        grow = jnp.exp(cum)
        weight = jnp.exp(total - cum) * step
        for group in range(groups):
            lanes = slice(group * STATE, (group + 1) * STATE)
            channels = slice(group * per_group * HEAD_DIM, (group + 1) * per_group * HEAD_DIM)
            b_blk, c_blk = b_all[rows, lanes], c_out[rows, lanes]
            scores = dot(c_blk, b_blk, ((1,), (1,)))
            if start > 0:
                read = dot(c_blk, entering[:, channels].astype(BF16)) * spread(grow, matrix[:, channels])
            for pair in range(per_group // 2):
                first = (group * per_group + 2 * pair) * HEAD_DIM
                results = []
                for head in (group * per_group + 2 * pair, group * per_group + 2 * pair + 1):
                    difference = turned[:, head : head + 1] - cum[head : head + 1, :]
                    decay = jnp.exp(jnp.where(keep, difference, -jnp.inf))
                    mixing = (scores * decay * step[head : head + 1, :]).astype(BF16)
                    results.append(dot(mixing, x_blk[:, first : first + 2 * HEAD_DIM]))
                y = jnp.where(left, results[0], results[1])
                if start > 0:
                    y = y + read[:, 2 * pair * HEAD_DIM : 2 * (pair + 1) * HEAD_DIM]
                y_out[rows, first : first + 2 * HEAD_DIM] = y * gate[rows, first : first + 2 * HEAD_DIM]
            if start + BLOCK < span:
                weighted = (x_blk[:, channels].astype(F32) * spread(weight, matrix[:, channels])).astype(BF16)
                added = dot(b_blk, weighted, ((0,), (0,)))
                if start > 0:
                    grown = spread(jnp.broadcast_to(jnp.exp(total), (heads, BLOCK)), matrix[:, channels], 3)
                    added = entering[:, channels] * grown + added
                entering[:, channels] = added


def output_kernel(own, y_in, grow, c_all, gain, p0, p1, p2, p3, out, ends):
    span, inner = y_in.shape
    groups = c_all.shape[1] // STATE
    quarter = inner // QUAD
    half = span // 2
    core = lax.axis_index("tp")
    rows = pl.ds(pl.multiple_of((core if own else 1 - core) * half, 64), half)
    me = lax.rem(lax.axis_index("sp"), QUAD)
    for bits, ref in enumerate((p0, p1, p2, p3)):
        ends[:, pl.ds(pl.multiple_of((me ^ bits) * quarter, 128), quarter)] = ref[...]
    place = lax.broadcasted_iota(jnp.int32, (quarter, quarter), 0) // HEAD_DIM
    same = place == lax.broadcasted_iota(jnp.int32, (quarter, quarter), 1) // HEAD_DIM
    mean = (same.astype(F32) * (1.0 / HEAD_DIM)).astype(BF16)
    for start in range(0, inner, quarter):
        lanes = slice(start, start + quarter)
        group = start // (inner // groups)
        read = dot(c_all[rows, group * STATE : (group + 1) * STATE], ends[:, lanes])
        gated = y_in[rows, lanes] + read * grow[rows, lanes]
        square = sum(dot(part, mean) for part in parts_of(gated * gated, 2))
        out[:, lanes] = (gated * lax.rsqrt(square + EPS) * gain[:, lanes].astype(F32)).astype(BF16)


def own_kernel(mine, w_own, out):
    out[...] = dot(mine[...], w_own[...])


def sum_kernel(own, other, w_other, out):
    out[...] = (own[...] + dot(other[...], w_other[...])).astype(BF16)


def tail_kernel(values, b_in, c_in, out, sems):
    offset, copies = 0, []
    for turn, source in enumerate((b_in, c_in, values)):
        rows, lanes = pl.ds(source.shape[0] - EDGE, EDGE), pl.ds(offset, source.shape[1])
        copies.append(pltpu.make_async_copy(source.at[rows, :], out.at[:, lanes], sems.at[turn]))
        offset += source.shape[1]
    for copy in copies:
        copy.start()
    for copy in copies:
        copy.wait()


def body(
    gate_in, values_in, input_state_in, output_state_in, step_in, conv_x, conv_b, conv_c, dt_bias, decay_rate, log_decay_extra,
    out_gain, w_out,
):
    span, inner = values_in.shape
    shared = input_state_in.shape[1]
    heads = step_in.shape[1]
    places = lax.axis_size("sp")
    quarter = inner // QUAD
    shape = jax.ShapeDtypeStruct
    vmem = pltpu.VMEM

    def move(x, route):
        return lax.ppermute(x, "sp", route)

    def exchange(x, bits, count=places):
        return move(x, [(i, i ^ bits) for i in range(count)])

    def edge_specs(block):
        return [pl.BlockSpec((EDGE, a.shape[1]), lambda i: (block, 0)) for a in (values_in, input_state_in, output_state_in)]

    tail = pl.pallas_call(
        tail_kernel,
        out_shape=shape((EDGE, inner + 2 * shared), BF16),
        in_specs=[pl.BlockSpec(memory_space=pl.ANY)] * 3,
        out_specs=whole(1)[0],
        scratch_shapes=[pltpu.SemaphoreType.DMA((3,))],
        compiler_params=pltpu.CompilerParams(vmem_limit_bytes=SMALL),
        name="tail",
    )(*(pltpu.with_memory_space_constraint(a, pltpu.HBM) for a in (values_in, input_state_in, output_state_in)))
    halo = move(tail, [(i, i + 1) for i in range(places - 1)])

    args = [
        values_in, input_state_in, output_state_in, step_in.T, log_decay_extra.T, conv_x, conv_b, conv_c,
        dt_bias.reshape(1, heads), decay_rate.reshape(1, heads),
    ]
    outs = [
        shape((span, inner), BF16), shape((span, shared), BF16), shape((span, shared), BF16), shape((heads, span), F32),
        shape((heads, span), F32), shape((STATE, inner), F32), shape((EXTRA, inner), BF16), shape((EDGE, inner), F32),
    ]
    x_act, b_act, c_act, cum, step, state, logs, edge_weight = pl.pallas_call(
        local_kernel,
        out_shape=outs,
        in_specs=[pl.BlockSpec(memory_space=pltpu.HBM)] * len(args),
        out_specs=whole(len(outs)),
        scratch_shapes=[vmem((span + 8, 256), F32)] + [vmem(a.shape, a.dtype) for a in args] + [pltpu.SemaphoreType.DMA((len(args),))],
        compiler_params=pltpu.CompilerParams(vmem_limit_bytes=LARGE),
        cost_estimate=pl.CostEstimate(flops=FILL, bytes_accessed=4_000_000, transcendentals=0),
        name="local",
    )(*(pltpu.with_memory_space_constraint(a, pltpu.HBM) for a in args))
    w_other, _ = lax.optimization_barrier((w_out, logs))
    w_other = lax.ppermute(w_other, "tp", [(0, 1), (1, 0)])
    payload = shape((STATE + EXTRA, quarter), BF16)
    edge_x, edge_b, edge_c, *slots = pl.pallas_call(
        edge_kernel,
        out_shape=[
            shape((EDGE, inner), BF16), shape((EDGE, shared), BF16), shape((EDGE, shared), BF16), payload, payload, payload, payload,
        ],
        grid=(1,),
        in_specs=edge_specs(0) + whole(7),
        out_specs=whole(7),
        scratch_shapes=[vmem((2 * EDGE, inner + 2 * shared), F32), vmem((STATE + EXTRA, inner), BF16)],
        compiler_params=pltpu.CompilerParams(vmem_limit_bytes=SMALL),
        name="edge",
    )(values_in, input_state_in, output_state_in, halo, conv_x, conv_b, conv_c, state, logs, edge_weight)
    gate, grow = local_call(gate_kernel, [shape((span, inner), F32)] * 2, [gate_in, cum], flops=FILL)
    y_inside, c_all = local_call(
        inside_kernel,
        [shape((span, inner), F32), shape((span, shared), BF16)],
        [x_act, b_act, c_act, edge_x, edge_b, edge_c, cum, step, gate],
        [
            vmem((span, shared), BF16), vmem((BLOCK, inner), BF16), vmem((BLOCK, BLOCK), F32), vmem((BLOCK, BLOCK), F32),
            vmem((STATE, inner), F32),
        ],
        flops=FILL,
    )

    order = vmem((QUAD, STATE + EXTRA, quarter), BF16)
    arrived = {bits: exchange(slots[bits], bits) for bits in (3, 2, 1)}
    quad = [slots[0], arrived[1], arrived[2], arrived[3]]
    slice_of = shape((STATE, quarter), BF16)
    kept = [shape((STATE, quarter), F32), shape((1, quarter), F32)]
    sent, total, log = local_call(quad_total_kernel, [payload, *kept], quad, [order], limit=SMALL)
    half = places // QUAD // 2

    def up(x, sources, fours):
        return move(x, [(i, i + fours * QUAD) for four in sources for i in range(four * QUAD, (four + 1) * QUAD)])

    passed = []
    for turn in range(half - 1):
        if turn:
            sent = local_call(functools.partial(hop_kernel, half, turn), payload, [passed[-1], total, log], limit=SMALL)
        passed.append(up(sent, (turn, half + turn), 1))
    lower = local_call(functools.partial(top_kernel, half), slice_of, [passed[-1], total, log], limit=SMALL)
    second = up(lower, (half - 1,), 2)
    fourth = up(lower, (half - 1,), 4)
    relayed = local_call(functools.partial(relay_kernel, half), slice_of, [lower, second], limit=SMALL)
    first = up(relayed, (half - 1, half + 1), 1)
    ends = local_call(
        functools.partial(prefix_kernel, half),
        [slice_of] * QUAD,
        [*passed, second, fourth, first, *quad],
        [order, vmem((QUAD, STATE, quarter), BF16), vmem(payload.shape, BF16), vmem(slice_of.shape, BF16)],
        limit=SMALL,
    )
    carried = {bits: exchange(ends[bits], bits) for bits in (3, 2, 1)}

    def normalized(own):
        return local_call(
            functools.partial(output_kernel, own),
            shape((span // 2, inner), BF16),
            [y_inside, grow, c_all, out_gain.reshape(1, inner), ends[0], carried[1], carried[2], carried[3]],
            [vmem((STATE, inner), BF16)],
        )

    theirs = normalized(False)
    other_rows = lax.ppermute(theirs, "tp", [(0, 1), (1, 0)])
    mine = normalized(True)
    wide = shape((span // 2, w_out.shape[1]), F32)
    own = local_call(own_kernel, wide, [mine, w_out], flops=FILL)
    return local_call(sum_kernel, shape(wide.shape, BF16), [own, other_rows, w_other])


def solution(mesh):
    rows = P(("grp", "sp"), "tp")
    placed = (rows, rows, rows, rows, rows, P(None, "tp"), P(None, "tp"), P(None, "tp"), P("tp"), P("tp"), rows, P("tp"), P("tp", None))
    return jax.shard_map(body, mesh=mesh, in_specs=placed, out_specs=P(("grp", "sp", "tp"), None), check_vma=False)
```

```python
import functools

import jax
import jax.numpy as jnp
from jax import lax
from jax.experimental import pallas as pl
from jax.experimental.pallas import tpu as pltpu
from jax.sharding import PartitionSpec as P


HEAD_DIM = 64
STATE = 128
CONV = 4
BLOCK = 128
QUAD = 4
EXTRA = 16
EPS = 1e-05
F32 = jnp.float32
BF16 = jnp.bfloat16
EDGE = 16
FILL = 4_000_000_000
SMALL = 4 * 1024 * 1024
LARGE = 16 * 1024 * 1024


def dot(a, b, dims=((1,), (0,))):
    return lax.dot_general(a, b, (dims, ((), ())), preferred_element_type=F32)


def parts_of(x, count):
    out = []
    for _ in range(count):
        part = x.astype(BF16)
        out.append(part)
        x = x - part.astype(F32)
    return out


def spread_matrix(heads):
    row = lax.broadcasted_iota(jnp.int32, (heads, heads * HEAD_DIM), 0)
    col = lax.broadcasted_iota(jnp.int32, (heads, heads * HEAD_DIM), 1)
    return (row == col // HEAD_DIM).astype(F32).astype(BF16)


def spread(x, matrix, count=2):
    return dot(jnp.concatenate(parts_of(x, count), axis=0), jnp.concatenate([matrix] * count, axis=0), ((0,), (0,)))


def column(row):
    size = row.shape[1]
    same = lax.broadcasted_iota(jnp.int32, (size, size), 0) == lax.broadcasted_iota(jnp.int32, (size, size), 1)
    return jnp.sum(jnp.where(same, row, 0.0), axis=1, keepdims=True)


def softplus(x):
    return jnp.maximum(x, 0.0) + jnp.log1p(jnp.exp(-jnp.abs(x)))


def silu(x):
    return x / (1.0 + jnp.exp(-x))


def convolved(ext, first, rows, taps):
    summed = jnp.zeros((rows, ext.shape[1]), F32)
    for tap in range(CONV):
        summed = summed + taps[tap : tap + 1].astype(F32) * ext[first + tap : first + tap + rows, :]
    return silu(summed).astype(BF16)


def local_kernel(
    values_hbm, b_hbm, c_hbm, step_hbm, extra_hbm, conv_x_hbm, conv_b_hbm, conv_c_hbm, dt_hbm, rate_hbm,
    x_act, b_act, c_act, cum_out, step_out, state_out, logs_out, edge_weight,
    ext, values, b_in, c_in, step_in, extra, conv_x, conv_b, conv_c, dt_bias, rate, sems,
):
    sources = (step_hbm, extra_hbm, dt_hbm, rate_hbm, b_hbm, conv_b_hbm, c_hbm, conv_c_hbm, values_hbm, conv_x_hbm)
    targets = (step_in, extra, dt_bias, rate, b_in, conv_b, c_in, conv_c, values, conv_x)
    copies = [pltpu.make_async_copy(source, target, sems.at[turn]) for turn, (source, target) in enumerate(zip(sources, targets, strict=True))]
    for copy in copies:
        copy.start()
    for copy in copies[:4]:
        copy.wait()
    span, inner = values.shape
    heads = step_in.shape[0]
    step = softplus(step_in[...].astype(F32) + column(dt_bias[...]))
    log_step = extra[...] - step * column(rate[...])
    step_out[...] = step
    row = lax.broadcasted_iota(jnp.int32, (BLOCK, BLOCK), 0)
    upper = (row <= lax.broadcasted_iota(jnp.int32, (BLOCK, BLOCK), 1)).astype(F32).astype(BF16)
    total = jnp.zeros((heads, 1), F32)
    for start in range(0, span, BLOCK):
        summed = dot(jnp.concatenate(parts_of(log_step[:, start : start + BLOCK], 3), axis=0), upper)
        cum = summed[:heads] + summed[heads : 2 * heads] + summed[2 * heads :] + total
        cum_out[:, start : start + BLOCK] = cum
        total = cum[:, BLOCK - 1 :]
    matrix = spread_matrix(heads)
    weight = jnp.exp(total - cum_out[...]) * step
    edge_weight[...] = spread(weight[:, 0:BLOCK], matrix)[0:EDGE]
    lane = lax.broadcasted_iota(jnp.int32, (heads, BLOCK), 1)
    high, middle, low = (part.astype(F32) for part in parts_of(total, 3))
    logs = jnp.where(lane == 0, high, jnp.where(lane == 1, middle, jnp.where(lane == 2, low, 0.0)))
    logs_out[...] = dot(logs.astype(BF16), matrix, ((0,), (0,)))[0:EXTRA].astype(BF16)
    weight = jnp.where(lax.broadcasted_iota(jnp.int32, (heads, span), 1) < EDGE, 0.0, weight)
    width = ext.shape[1]
    ext[0:8, :] = jnp.zeros((8, width), F32)
    per_group = inner // (b_in.shape[1] // STATE)
    for turn, (source, taps, target) in enumerate(((b_in, conv_b, b_act), (c_in, conv_c, c_act), (values, conv_x, x_act))):
        for copy in copies[4 + 2 * turn : 6 + 2 * turn]:
            copy.wait()
        for start in range(0, source.shape[1], width):
            lanes = slice(start, start + width)
            ext[8 : 8 + span, :] = source[:, lanes].astype(F32)
            active = convolved(ext, 8 - (CONV - 1), span, taps[:, lanes])
            target[:, lanes] = active
            if source is values:
                group = start // per_group
                weighted = (active.astype(F32) * spread(weight, matrix[:, lanes])).astype(BF16)
                state_out[:, lanes] = dot(b_act[:, group * STATE : (group + 1) * STATE], weighted, ((0,), (0,)))


def edge_kernel(
    values, b_in, c_in, halo, conv_x, conv_b, conv_c, state_in, logs_in, edge_weight,
    edge_x, edge_b, edge_c, slot0, slot1, slot2, slot3, ext, packed,
):
    inner, shared = values.shape[1], b_in.shape[1]
    offset = 0
    for source, taps, target in ((b_in, conv_b, edge_b), (c_in, conv_c, edge_c), (values, conv_x, edge_x)):
        lanes = slice(offset, offset + source.shape[1])
        part = ext.at[:, lanes]
        part[0:EDGE, :] = halo[:, lanes].astype(F32)
        part[EDGE : 2 * EDGE, :] = source[...].astype(F32)
        target[...] = convolved(part, EDGE - (CONV - 1), EDGE, taps[...])
        offset += source.shape[1]
    groups = shared // STATE
    weighted = (edge_x[...].astype(F32) * edge_weight[...]).astype(BF16)
    for group in range(groups):
        lanes = slice(group * (inner // groups), (group + 1) * (inner // groups))
        added = dot(edge_b[:, group * STATE : (group + 1) * STATE], weighted[:, lanes], ((0,), (0,)))
        packed[0:STATE, lanes] = (state_in[:, lanes] + added).astype(BF16)
    packed[STATE:, :] = logs_in[...]
    me = lax.rem(lax.axis_index("sp"), QUAD)
    quarter = inner // QUAD
    for bits, slot in enumerate((slot0, slot1, slot2, slot3)):
        slot[...] = packed[:, pl.ds(pl.multiple_of((me ^ bits) * quarter, 128), quarter)]


def whole(count):
    return [pl.BlockSpec(memory_space=pltpu.VMEM)] * count


def local_call(kernel, outs, args, scratch=(), flops=0, limit=None):
    many = isinstance(outs, (list, tuple))
    size = sum(a.size * a.dtype.itemsize for a in args)
    return pl.pallas_call(
        kernel,
        out_shape=outs,
        in_specs=whole(len(args)),
        out_specs=whole(len(outs)) if many else whole(1)[0],
        scratch_shapes=list(scratch),
        compiler_params=pltpu.CompilerParams(vmem_limit_bytes=limit or LARGE),
        cost_estimate=pl.CostEstimate(flops=flops, bytes_accessed=size, transcendentals=0),
    )(*args)


def load(ref):
    logs = ref[STATE:, :].astype(F32)
    return ref[0:STATE, :].astype(F32), logs[0:1] + logs[1:2] + logs[2:3]


def quad_order(ordered, refs):
    me = lax.rem(lax.axis_index("sp"), QUAD)
    for bits, ref in enumerate(refs):
        ordered[me ^ bits] = ref[...]


def store(ref, state, log):
    ref[0:STATE, :] = state.astype(BF16)
    high, middle, low = (part.astype(F32) for part in parts_of(log, 3))
    row = lax.broadcasted_iota(jnp.int32, (EXTRA, log.shape[1]), 0)
    logs = jnp.where(row == 0, high, jnp.where(row == 1, middle, jnp.where(row == 2, low, 0.0)))
    ref[STATE:, :] = logs.astype(BF16)


def quad_total_kernel(own, r1, r2, r3, sent, state_out, log_out, ordered):
    quad_order(ordered, (own, r1, r2, r3))
    state, log = load(ordered.at[0])
    for place in range(1, QUAD):
        part, part_log = load(ordered.at[place])
        state, log = state * jnp.exp(part_log) + part, log + part_log
    store(sent, state, log)
    state_out[...] = state
    log_out[...] = log


def jump_kernel(four, before, last, total, total_log, out):
    @pl.when(lax.axis_index("sp") // QUAD == four)
    def _():
        state = before[0:STATE, :].astype(F32)
        if last is not None:
            part, log = load(last)
            state = state * jnp.exp(log) + part
        out[...] = (state * jnp.exp(total_log[...]) + total[...]).astype(BF16)


def prefix_kernel(targets, *refs):
    ordered, ends, held, got = refs[-4:]
    quad, outs = refs[-12:-8], refs[-8:-4]
    arrived, pairs = refs[:-13], refs[-13]
    place = lax.axis_index("sp")
    group = place // QUAD
    quad_order(ordered, quad)
    held[...] = jnp.zeros_like(held)
    got[...] = jnp.zeros_like(got)
    for target, ref in zip(targets, arrived, strict=True):

        @pl.when(group == target)
        def _(ref=ref):
            got[...] = ref[0:STATE, :]

    @pl.when(jnp.logical_and(group > max(targets) // 2, lax.rem(group, 2) == 1))
    def _():
        held[...] = pairs[...]

    state, log = load(held)
    state = got[...].astype(F32) * jnp.exp(log) + state
    ends[0] = state.astype(BF16)
    for turn in range(QUAD - 1):
        part, log = load(ordered.at[turn])
        state = state * jnp.exp(log) + part
        ends[turn + 1] = state.astype(BF16)
    me = lax.rem(place, QUAD)
    for bits, out in enumerate(outs):
        out[...] = ends[me ^ bits]


def gate_kernel(gate, cum_all, gate_out, grow_out):
    matrix = spread_matrix(cum_all.shape[0])
    width = 256
    grow = jnp.exp(cum_all[...])
    for start in range(0, gate.shape[1], width):
        lanes = slice(start, start + width)
        gated = silu(gate[:, lanes].astype(F32))
        gate_out[:, lanes] = gated
        grow_out[:, lanes] = gated * spread(grow, matrix[:, lanes])


def inside_kernel(
    x_act, b_act, c_act, edge_x, edge_b, edge_c, cum_all, step_all, gate,
    y_out, c_out, b_all, x_first, padded, turned, entering,
):
    span, _ = x_act.shape
    heads = step_all.shape[0]
    groups = b_act.shape[1] // STATE
    per_group = heads // groups
    matrix = spread_matrix(heads)
    keep = lax.broadcasted_iota(jnp.int32, (BLOCK, BLOCK), 0) >= lax.broadcasted_iota(jnp.int32, (BLOCK, BLOCK), 1)
    left = lax.broadcasted_iota(jnp.int32, (BLOCK, 2 * HEAD_DIM), 1) < HEAD_DIM
    c_out[...] = c_act[...]
    c_out[0:EDGE, :] = edge_c[...]
    b_all[...] = b_act[...]
    b_all[0:EDGE, :] = edge_b[...]
    x_first[...] = x_act[0:BLOCK, :]
    x_first[0:EDGE, :] = edge_x[...]
    padded[...] = jnp.zeros_like(padded)
    before = jnp.zeros((heads, 1), F32)
    for start in range(0, span, BLOCK):
        rows = slice(start, start + BLOCK)
        x_blk = x_first if start == 0 else x_act.at[rows]
        cum = cum_all[:, rows] - before
        step = step_all[:, rows]
        padded[0:heads, :] = cum
        turned[...] = jnp.transpose(padded[...])
        total = cum[:, BLOCK - 1 :]
        before = before + total
        grow = jnp.exp(cum)
        weight = jnp.exp(total - cum) * step
        for group in range(groups):
            lanes = slice(group * STATE, (group + 1) * STATE)
            channels = slice(group * per_group * HEAD_DIM, (group + 1) * per_group * HEAD_DIM)
            b_blk, c_blk = b_all[rows, lanes], c_out[rows, lanes]
            scores = dot(c_blk, b_blk, ((1,), (1,)))
            if start > 0:
                read = dot(c_blk, entering[:, channels].astype(BF16)) * spread(grow, matrix[:, channels])
            for pair in range(per_group // 2):
                first = (group * per_group + 2 * pair) * HEAD_DIM
                results = []
                for head in (group * per_group + 2 * pair, group * per_group + 2 * pair + 1):
                    difference = turned[:, head : head + 1] - cum[head : head + 1, :]
                    decay = jnp.exp(jnp.where(keep, difference, -jnp.inf))
                    mixing = (scores * decay * step[head : head + 1, :]).astype(BF16)
                    results.append(dot(mixing, x_blk[:, first : first + 2 * HEAD_DIM]))
                y = jnp.where(left, results[0], results[1])
                if start > 0:
                    y = y + read[:, 2 * pair * HEAD_DIM : 2 * (pair + 1) * HEAD_DIM]
                y_out[rows, first : first + 2 * HEAD_DIM] = y * gate[rows, first : first + 2 * HEAD_DIM]
            if start + BLOCK < span:
                weighted = (x_blk[:, channels].astype(F32) * spread(weight, matrix[:, channels])).astype(BF16)
                added = dot(b_blk, weighted, ((0,), (0,)))
                if start > 0:
                    grown = spread(jnp.broadcast_to(jnp.exp(total), (heads, BLOCK)), matrix[:, channels], 3)
                    added = entering[:, channels] * grown + added
                entering[:, channels] = added


def output_kernel(own, y_in, grow, c_all, gain, p0, p1, p2, p3, w_out, out, ends, normalized):
    span, inner = y_in.shape
    groups = c_all.shape[1] // STATE
    quarter = inner // QUAD
    half = span // 2
    core = lax.axis_index("tp")
    rows = pl.ds(pl.multiple_of((core if own else 1 - core) * half, 64), half)
    me = lax.rem(lax.axis_index("sp"), QUAD)
    for bits, ref in enumerate((p0, p1, p2, p3)):
        ends[:, pl.ds(pl.multiple_of((me ^ bits) * quarter, 128), quarter)] = ref[...]
    place = lax.broadcasted_iota(jnp.int32, (quarter, quarter), 0) // HEAD_DIM
    same = place == lax.broadcasted_iota(jnp.int32, (quarter, quarter), 1) // HEAD_DIM
    mean = (same.astype(F32) * (1.0 / HEAD_DIM)).astype(BF16)
    for start in range(0, inner, quarter):
        lanes = slice(start, start + quarter)
        group = start // (inner // groups)
        read = dot(c_all[rows, group * STATE : (group + 1) * STATE], ends[:, lanes])
        gated = y_in[rows, lanes] + read * grow[rows, lanes]
        square = sum(dot(part, mean) for part in parts_of(gated * gated, 2))
        normalized[:, lanes] = (gated * lax.rsqrt(square + EPS) * gain[:, lanes].astype(F32)).astype(BF16)
    width = 512
    for start in range(0, w_out.shape[1], width):
        lanes = slice(start, start + width)
        out[:, lanes] = dot(normalized[...], w_out[:, lanes]).astype(out.dtype)


def sum_kernel(own, other, out):
    out[...] = (own[...] + other[...].astype(F32)).astype(BF16)


def tail_kernel(values, b_in, c_in, out, sems):
    offset, copies = 0, []
    for turn, source in enumerate((b_in, c_in, values)):
        rows, lanes = pl.ds(source.shape[0] - EDGE, EDGE), pl.ds(offset, source.shape[1])
        copies.append(pltpu.make_async_copy(source.at[rows, :], out.at[:, lanes], sems.at[turn]))
        offset += source.shape[1]
    for copy in copies:
        copy.start()
    for copy in copies:
        copy.wait()


def body(
    gate_in, values_in, input_state_in, output_state_in, step_in, conv_x, conv_b, conv_c, dt_bias, decay_rate, log_decay_extra,
    out_gain, w_out,
):
    span, inner = values_in.shape
    shared = input_state_in.shape[1]
    heads = step_in.shape[1]
    places = lax.axis_size("sp")
    quarter = inner // QUAD
    shape = jax.ShapeDtypeStruct
    vmem = pltpu.VMEM

    def move(x, route):
        return lax.ppermute(x, "sp", route)

    def exchange(x, bits, count=places):
        return move(x, [(i, i ^ bits) for i in range(count)])

    def edge_specs(block):
        return [pl.BlockSpec((EDGE, a.shape[1]), lambda i: (block, 0)) for a in (values_in, input_state_in, output_state_in)]

    tail = pl.pallas_call(
        tail_kernel,
        out_shape=shape((EDGE, inner + 2 * shared), BF16),
        in_specs=[pl.BlockSpec(memory_space=pl.ANY)] * 3,
        out_specs=whole(1)[0],
        scratch_shapes=[pltpu.SemaphoreType.DMA((3,))],
        compiler_params=pltpu.CompilerParams(vmem_limit_bytes=SMALL),
        name="tail",
    )(*(pltpu.with_memory_space_constraint(a, pltpu.HBM) for a in (values_in, input_state_in, output_state_in)))
    halo = move(tail, [(i, i + 1) for i in range(places - 1)])

    args = [
        values_in, input_state_in, output_state_in, step_in.T, log_decay_extra.T, conv_x, conv_b, conv_c,
        dt_bias.reshape(1, heads), decay_rate.reshape(1, heads),
    ]
    outs = [
        shape((span, inner), BF16), shape((span, shared), BF16), shape((span, shared), BF16), shape((heads, span), F32),
        shape((heads, span), F32), shape((STATE, inner), F32), shape((EXTRA, inner), BF16), shape((EDGE, inner), F32),
    ]
    x_act, b_act, c_act, cum, step, state, logs, edge_weight = pl.pallas_call(
        local_kernel,
        out_shape=outs,
        in_specs=[pl.BlockSpec(memory_space=pltpu.HBM)] * len(args),
        out_specs=whole(len(outs)),
        scratch_shapes=[vmem((span + 8, 256), F32)] + [vmem(a.shape, a.dtype) for a in args] + [pltpu.SemaphoreType.DMA((len(args),))],
        compiler_params=pltpu.CompilerParams(vmem_limit_bytes=LARGE),
        cost_estimate=pl.CostEstimate(flops=FILL, bytes_accessed=4_000_000, transcendentals=0),
        name="local",
    )(*(pltpu.with_memory_space_constraint(a, pltpu.HBM) for a in args))
    payload = shape((STATE + EXTRA, quarter), BF16)
    edge_x, edge_b, edge_c, *slots = pl.pallas_call(
        edge_kernel,
        out_shape=[
            shape((EDGE, inner), BF16), shape((EDGE, shared), BF16), shape((EDGE, shared), BF16), payload, payload, payload, payload,
        ],
        grid=(1,),
        in_specs=edge_specs(0) + whole(7),
        out_specs=whole(7),
        scratch_shapes=[vmem((2 * EDGE, inner + 2 * shared), F32), vmem((STATE + EXTRA, inner), BF16)],
        compiler_params=pltpu.CompilerParams(vmem_limit_bytes=SMALL),
        name="edge",
    )(values_in, input_state_in, output_state_in, halo, conv_x, conv_b, conv_c, state, logs, edge_weight)
    gate, grow = local_call(gate_kernel, [shape((span, inner), F32)] * 2, [gate_in, cum], flops=FILL)
    y_inside, c_all = local_call(
        inside_kernel,
        [shape((span, inner), F32), shape((span, shared), BF16)],
        [x_act, b_act, c_act, edge_x, edge_b, edge_c, cum, step, gate],
        [
            vmem((span, shared), BF16), vmem((BLOCK, inner), BF16), vmem((BLOCK, BLOCK), F32), vmem((BLOCK, BLOCK), F32),
            vmem((STATE, inner), F32),
        ],
        flops=FILL,
    )

    order = vmem((QUAD, STATE + EXTRA, quarter), BF16)
    arrived = {bits: exchange(slots[bits], bits) for bits in (3, 2, 1)}
    quad = [slots[0], arrived[1], arrived[2], arrived[3]]
    slice_of = shape((STATE, quarter), BF16)
    kept = [shape((STATE, quarter), F32), shape((1, quarter), F32)]
    sent, total, log = local_call(quad_total_kernel, [payload, *kept], quad, [order], limit=SMALL)
    fours = places // QUAD
    half = fours // 2

    def up(x, sources, distance):
        return move(x, [(i, i + distance * QUAD) for four in sources for i in range(four * QUAD, (four + 1) * QUAD)])

    def jump(four, before, last=None):
        if last is None:
            kernel = lambda *refs: jump_kernel(four, refs[0], None, *refs[1:])
            return local_call(kernel, slice_of, [before, total, log], limit=SMALL)
        return local_call(functools.partial(jump_kernel, four), slice_of, [before, last, total, log], limit=SMALL)

    pairs = up(sent, range(half, fours, 2), 1)
    arrived, targets = [], []

    def send(x, four, distance):
        arrived.append(up(x, (four,), distance))
        targets.append(four + distance)
        return arrived[-1]

    before = send(sent, 0, 1)
    for four in range(1, half - 1):
        before = send(jump(four, before), four, 1)
    lower = jump(half - 1, before)
    for four in range(half - 1, fours - 1, 2):
        before = send(lower, four, 2)
        send(lower, four, 1)
        if four + 2 < fours - 1:
            lower = jump(four + 2, before, pairs)
    ends = local_call(
        functools.partial(prefix_kernel, tuple(targets)),
        [slice_of] * QUAD,
        [*arrived, pairs, *quad],
        [order, vmem((QUAD, STATE, quarter), BF16), vmem(payload.shape, BF16), vmem(slice_of.shape, BF16)],
        limit=SMALL,
    )
    carried = {bits: exchange(ends[bits], bits) for bits in (3, 2, 1)}

    def projected(own):
        return local_call(
            functools.partial(output_kernel, own),
            shape((span // 2, w_out.shape[1]), F32 if own else BF16),
            [y_inside, grow, c_all, out_gain.reshape(1, inner), ends[0], carried[1], carried[2], carried[3], w_out],
            [vmem((STATE, inner), BF16), vmem((span // 2, inner), BF16)],
            flops=FILL,
        )

    theirs = projected(False)
    other = lax.ppermute(theirs, "tp", [(0, 1), (1, 0)])
    mine = projected(True)
    return local_call(sum_kernel, shape(mine.shape, BF16), [mine, other])


def solution(mesh):
    rows = P(("grp", "sp"), "tp")
    placed = (rows, rows, rows, rows, rows, P(None, "tp"), P(None, "tp"), P(None, "tp"), P("tp"), P("tp"), rows, P("tp"), P("tp", None))
    return jax.shard_map(body, mesh=mesh, in_specs=placed, out_specs=P(("grp", "sp", "tp"), None), check_vma=False)
```

```python
import functools

import jax
import jax.numpy as jnp
from jax import lax
from jax.experimental import pallas as pl
from jax.experimental.pallas import tpu as pltpu
from jax.sharding import PartitionSpec as P


HEAD_DIM = 64
STATE = 128
CONV = 4
BLOCK = 128
QUAD = 4
EXTRA = 16
EPS = 1e-05
F32 = jnp.float32
BF16 = jnp.bfloat16
EDGE = 16
FILL = 4_000_000_000
SMALL = 4 * 1024 * 1024
LARGE = 16 * 1024 * 1024


def dot(a, b, dims=((1,), (0,))):
    return lax.dot_general(a, b, (dims, ((), ())), preferred_element_type=F32)


def parts_of(x, count):
    out = []
    for _ in range(count):
        part = x.astype(BF16)
        out.append(part)
        x = x - part.astype(F32)
    return out


def spread_matrix(heads):
    row = lax.broadcasted_iota(jnp.int32, (heads, heads * HEAD_DIM), 0)
    col = lax.broadcasted_iota(jnp.int32, (heads, heads * HEAD_DIM), 1)
    return (row == col // HEAD_DIM).astype(F32).astype(BF16)


def spread(x, matrix, count=2):
    return dot(jnp.concatenate(parts_of(x, count), axis=0), jnp.concatenate([matrix] * count, axis=0), ((0,), (0,)))


def column(row):
    size = row.shape[1]
    same = lax.broadcasted_iota(jnp.int32, (size, size), 0) == lax.broadcasted_iota(jnp.int32, (size, size), 1)
    return jnp.sum(jnp.where(same, row, 0.0), axis=1, keepdims=True)


def softplus(x):
    return jnp.maximum(x, 0.0) + jnp.log1p(jnp.exp(-jnp.abs(x)))


def silu(x):
    half = 0.5 * x
    return half + half * jnp.tanh(half)


def convolved(ext, first, rows, taps):
    summed = jnp.zeros((rows, ext.shape[1]), F32)
    for tap in range(CONV):
        summed = summed + taps[tap : tap + 1].astype(F32) * ext[first + tap : first + tap + rows, :]
    return silu(summed).astype(BF16)


def local_kernel(
    values_hbm, b_hbm, c_hbm, step_hbm, extra_hbm, conv_x_hbm, conv_b_hbm, conv_c_hbm, dt_hbm, rate_hbm,
    x_act, b_act, c_act, cum_out, step_out, state_out, logs_out, edge_weight, head, tail,
    ext, values, b_in, c_in, step_in, extra, conv_x, conv_b, conv_c, dt_bias, rate, sems,
):
    sources = (step_hbm, extra_hbm, dt_hbm, rate_hbm, b_hbm, conv_b_hbm, c_hbm, conv_c_hbm, values_hbm, conv_x_hbm)
    targets = (step_in, extra, dt_bias, rate, b_in, conv_b, c_in, conv_c, values, conv_x)
    copies = [pltpu.make_async_copy(source, target, sems.at[turn]) for turn, (source, target) in enumerate(zip(sources, targets, strict=True))]
    for copy in copies:
        copy.start()
    for copy in copies[:4]:
        copy.wait()
    span, inner = values.shape
    heads = step_in.shape[0]
    step = softplus(step_in[...].astype(F32) + column(dt_bias[...]))
    log_step = extra[...] - step * column(rate[...])
    step_out[...] = step
    row = lax.broadcasted_iota(jnp.int32, (BLOCK, BLOCK), 0)
    upper = (row <= lax.broadcasted_iota(jnp.int32, (BLOCK, BLOCK), 1)).astype(F32).astype(BF16)
    total = jnp.zeros((heads, 1), F32)
    for start in range(0, span, BLOCK):
        summed = dot(jnp.concatenate(parts_of(log_step[:, start : start + BLOCK], 3), axis=0), upper)
        cum = summed[:heads] + summed[heads : 2 * heads] + summed[2 * heads :] + total
        cum_out[:, start : start + BLOCK] = cum
        total = cum[:, BLOCK - 1 :]
    matrix = spread_matrix(heads)
    weight = jnp.exp(total - cum_out[...]) * step
    edge_weight[...] = spread(weight[:, 0:BLOCK], matrix)[0:EDGE]
    lane = lax.broadcasted_iota(jnp.int32, (heads, BLOCK), 1)
    high, middle, low = (part.astype(F32) for part in parts_of(total, 3))
    logs = jnp.where(lane == 0, high, jnp.where(lane == 1, middle, jnp.where(lane == 2, low, 0.0)))
    logs_out[...] = dot(logs.astype(BF16), matrix, ((0,), (0,)))[0:EXTRA].astype(BF16)
    weight = jnp.where(lax.broadcasted_iota(jnp.int32, (heads, span), 1) < EDGE, 0.0, weight)
    width = ext.shape[1]
    ext[0:8, :] = jnp.zeros((8, width), F32)
    per_group = inner // (b_in.shape[1] // STATE)
    offset = 0
    for turn, (source, taps, target) in enumerate(((b_in, conv_b, b_act), (c_in, conv_c, c_act), (values, conv_x, x_act))):
        for copy in copies[4 + 2 * turn : 6 + 2 * turn]:
            copy.wait()
        head[:, offset : offset + source.shape[1]] = source[0:EDGE, :]
        tail[:, offset : offset + source.shape[1]] = source[span - EDGE :, :]
        offset += source.shape[1]
        for start in range(0, source.shape[1], width):
            lanes = slice(start, start + width)
            ext[8 : 8 + span, :] = source[:, lanes].astype(F32)
            active = convolved(ext, 8 - (CONV - 1), span, taps[:, lanes])
            target[:, lanes] = active
            if source is values:
                group = start // per_group
                weighted = (active.astype(F32) * spread(weight, matrix[:, lanes])).astype(BF16)
                state_out[:, lanes] = dot(b_act[:, group * STATE : (group + 1) * STATE], weighted, ((0,), (0,)))


def edge_kernel(
    head, halo, conv_x, conv_b, conv_c, state_in, logs_in, edge_weight,
    edge_x, edge_b, edge_c, slot0, slot1, slot2, slot3, ext, packed,
):
    inner, shared = edge_x.shape[1], edge_b.shape[1]
    ext[0:EDGE, :] = halo[...].astype(F32)
    ext[EDGE : 2 * EDGE, :] = head[...].astype(F32)
    offset = 0
    for taps, target in ((conv_b, edge_b), (conv_c, edge_c), (conv_x, edge_x)):
        lanes = slice(offset, offset + target.shape[1])
        target[...] = convolved(ext.at[:, lanes], EDGE - (CONV - 1), EDGE, taps[...])
        offset += target.shape[1]
    groups = shared // STATE
    weighted = (edge_x[...].astype(F32) * edge_weight[...]).astype(BF16)
    for group in range(groups):
        lanes = slice(group * (inner // groups), (group + 1) * (inner // groups))
        added = dot(edge_b[:, group * STATE : (group + 1) * STATE], weighted[:, lanes], ((0,), (0,)))
        packed[0:STATE, lanes] = (state_in[:, lanes] + added).astype(BF16)
    packed[STATE:, :] = logs_in[...]
    me = lax.rem(lax.axis_index("sp"), QUAD)
    quarter = inner // QUAD
    for bits, slot in enumerate((slot0, slot1, slot2, slot3)):
        slot[...] = packed[:, pl.ds(pl.multiple_of((me ^ bits) * quarter, 128), quarter)]


def whole(count):
    return [pl.BlockSpec(memory_space=pltpu.VMEM)] * count


def local_call(kernel, outs, args, scratch=(), flops=0, limit=None):
    many = isinstance(outs, (list, tuple))
    size = sum(a.size * a.dtype.itemsize for a in args)
    return pl.pallas_call(
        kernel,
        out_shape=outs,
        in_specs=whole(len(args)),
        out_specs=whole(len(outs)) if many else whole(1)[0],
        scratch_shapes=list(scratch),
        compiler_params=pltpu.CompilerParams(vmem_limit_bytes=limit or LARGE),
        cost_estimate=pl.CostEstimate(flops=flops, bytes_accessed=size, transcendentals=0),
    )(*args)


def load(ref):
    logs = ref[STATE:, :].astype(F32)
    return ref[0:STATE, :].astype(F32), logs[0:1] + logs[1:2] + logs[2:3]


def quad_order(ordered, refs):
    me = lax.rem(lax.axis_index("sp"), QUAD)
    for bits, ref in enumerate(refs):
        ordered[me ^ bits] = ref[...]


def store(ref, state, log):
    ref[0:STATE, :] = state.astype(BF16)
    high, middle, low = (part.astype(F32) for part in parts_of(log, 3))
    row = lax.broadcasted_iota(jnp.int32, (EXTRA, log.shape[1]), 0)
    logs = jnp.where(row == 0, high, jnp.where(row == 1, middle, jnp.where(row == 2, low, 0.0)))
    ref[STATE:, :] = logs.astype(BF16)


def quad_total_kernel(own, r1, r2, r3, first, sent, state_out, log_out, ordered):
    quad_order(ordered, (own, r1, r2, r3))
    state, log = load(ordered.at[0])
    for place in range(1, QUAD):
        part, part_log = load(ordered.at[place])
        state, log = state * jnp.exp(part_log) + part, log + part_log
    first[...] = state.astype(BF16)
    store(sent, state, log)
    state_out[...] = state
    log_out[...] = log


def jump_kernel(four, before, last, total, total_log, out):
    @pl.when(lax.axis_index("sp") // QUAD == four)
    def _():
        state = before[0:STATE, :].astype(F32)
        if last is not None:
            part, log = load(last)
            state = state * jnp.exp(log) + part
        out[...] = (state * jnp.exp(total_log[...]) + total[...]).astype(BF16)


def choose_kernel(fours, *refs):
    for four, ref in zip(fours, refs, strict=False):

        @pl.when(lax.axis_index("sp") // QUAD == four)
        def _(ref=ref):
            refs[-1][...] = ref[...]


def prefix_kernel(targets, *refs):
    ordered, ends, held, got = refs[-4:]
    quad, outs = refs[-12:-8], refs[-8:-4]
    arrived, pairs = refs[:-13], refs[-13]
    place = lax.axis_index("sp")
    group = place // QUAD
    quad_order(ordered, quad)
    held[...] = jnp.zeros_like(held)
    got[...] = jnp.zeros_like(got)
    for target, ref in zip(targets, arrived, strict=True):

        @pl.when(group == target)
        def _(ref=ref):
            got[...] = ref[0:STATE, :]

    @pl.when(jnp.logical_and(group > max(targets) // 2, lax.rem(group, 2) == 1))
    def _():
        held[...] = pairs[...]

    state, log = load(held)
    state = got[...].astype(F32) * jnp.exp(log) + state
    ends[0] = state.astype(BF16)
    for turn in range(QUAD - 1):
        part, log = load(ordered.at[turn])
        state = state * jnp.exp(log) + part
        ends[turn + 1] = state.astype(BF16)
    me = lax.rem(place, QUAD)
    for bits, out in enumerate(outs):
        out[...] = ends[me ^ bits]


def gate_kernel(gate, cum_all, gate_out, grow_out):
    matrix = spread_matrix(cum_all.shape[0])
    width = 256
    grow = jnp.exp(cum_all[...])
    for start in range(0, gate.shape[1], width):
        lanes = slice(start, start + width)
        gated = silu(gate[:, lanes].astype(F32))
        gate_out[:, lanes] = gated
        grow_out[:, lanes] = gated * spread(grow, matrix[:, lanes])


def inside_kernel(
    x_act, b_act, c_act, edge_x, edge_b, edge_c, cum_all, step_all, gate,
    y_out, c_out, b_all, x_first, padded, turned, entering,
):
    span, _ = x_act.shape
    heads = step_all.shape[0]
    groups = b_act.shape[1] // STATE
    per_group = heads // groups
    matrix = spread_matrix(heads)
    keep = lax.broadcasted_iota(jnp.int32, (BLOCK, BLOCK), 0) >= lax.broadcasted_iota(jnp.int32, (BLOCK, BLOCK), 1)
    left = lax.broadcasted_iota(jnp.int32, (BLOCK, 2 * HEAD_DIM), 1) < HEAD_DIM
    c_out[...] = c_act[...]
    c_out[0:EDGE, :] = edge_c[...]
    b_all[...] = b_act[...]
    b_all[0:EDGE, :] = edge_b[...]
    x_first[...] = x_act[0:BLOCK, :]
    x_first[0:EDGE, :] = edge_x[...]
    padded[...] = jnp.zeros_like(padded)
    before = jnp.zeros((heads, 1), F32)
    for start in range(0, span, BLOCK):
        rows = slice(start, start + BLOCK)
        x_blk = x_first if start == 0 else x_act.at[rows]
        cum = cum_all[:, rows] - before
        step = step_all[:, rows]
        padded[0:heads, :] = cum
        turned[...] = jnp.transpose(padded[...])
        total = cum[:, BLOCK - 1 :]
        before = before + total
        grow = jnp.exp(cum)
        weight = jnp.exp(total - cum) * step
        for group in range(groups):
            lanes = slice(group * STATE, (group + 1) * STATE)
            channels = slice(group * per_group * HEAD_DIM, (group + 1) * per_group * HEAD_DIM)
            b_blk, c_blk = b_all[rows, lanes], c_out[rows, lanes]
            scores = dot(c_blk, b_blk, ((1,), (1,)))
            if start > 0:
                read = dot(c_blk, entering[:, channels].astype(BF16)) * spread(grow, matrix[:, channels])
            for pair in range(per_group // 2):
                first = (group * per_group + 2 * pair) * HEAD_DIM
                results = []
                for head in (group * per_group + 2 * pair, group * per_group + 2 * pair + 1):
                    difference = turned[:, head : head + 1] - cum[head : head + 1, :]
                    decay = jnp.exp(jnp.where(keep, difference, -jnp.inf))
                    mixing = (scores * decay * step[head : head + 1, :]).astype(BF16)
                    results.append(dot(mixing, x_blk[:, first : first + 2 * HEAD_DIM]))
                y = jnp.where(left, results[0], results[1])
                if start > 0:
                    y = y + read[:, 2 * pair * HEAD_DIM : 2 * (pair + 1) * HEAD_DIM]
                y_out[rows, first : first + 2 * HEAD_DIM] = y * gate[rows, first : first + 2 * HEAD_DIM]
            if start + BLOCK < span:
                weighted = (x_blk[:, channels].astype(F32) * spread(weight, matrix[:, channels])).astype(BF16)
                added = dot(b_blk, weighted, ((0,), (0,)))
                if start > 0:
                    grown = spread(jnp.broadcast_to(jnp.exp(total), (heads, BLOCK)), matrix[:, channels], 3)
                    added = entering[:, channels] * grown + added
                entering[:, channels] = added


def output_kernel(own, y_in, grow, c_all, gain, p0, p1, p2, p3, w_out, out, ends, normalized):
    span, inner = y_in.shape
    groups = c_all.shape[1] // STATE
    quarter = inner // QUAD
    half = span // 2
    core = lax.axis_index("tp")
    rows = pl.ds(pl.multiple_of((core if own else 1 - core) * half, 64), half)
    me = lax.rem(lax.axis_index("sp"), QUAD)
    for bits, ref in enumerate((p0, p1, p2, p3)):
        ends[:, pl.ds(pl.multiple_of((me ^ bits) * quarter, 128), quarter)] = ref[...]
    place = lax.broadcasted_iota(jnp.int32, (quarter, quarter), 0) // HEAD_DIM
    same = place == lax.broadcasted_iota(jnp.int32, (quarter, quarter), 1) // HEAD_DIM
    mean = (same.astype(F32) * (1.0 / HEAD_DIM)).astype(BF16)
    for start in range(0, inner, quarter):
        lanes = slice(start, start + quarter)
        group = start // (inner // groups)
        read = dot(c_all[rows, group * STATE : (group + 1) * STATE], ends[:, lanes])
        gated = y_in[rows, lanes] + read * grow[rows, lanes]
        square = sum(dot(part, mean) for part in parts_of(gated * gated, 2))
        normalized[:, lanes] = (gated * lax.rsqrt(square + EPS) * gain[:, lanes].astype(F32)).astype(BF16)
    width = 512
    for start in range(0, w_out.shape[1], width):
        lanes = slice(start, start + width)
        out[:, lanes] = dot(normalized[...], w_out[:, lanes]).astype(out.dtype)


def sum_kernel(own, other, out):
    out[...] = (own[...] + other[...].astype(F32)).astype(BF16)


def body(
    gate_in, values_in, input_state_in, output_state_in, step_in, conv_x, conv_b, conv_c, dt_bias, decay_rate, log_decay_extra,
    out_gain, w_out,
):
    span, inner = values_in.shape
    shared = input_state_in.shape[1]
    heads = step_in.shape[1]
    places = lax.axis_size("sp")
    quarter = inner // QUAD
    shape = jax.ShapeDtypeStruct
    vmem = pltpu.VMEM

    def move(x, route):
        return lax.ppermute(x, "sp", route)

    def exchange(x, bits, count=places):
        return move(x, [(i, i ^ bits) for i in range(count)])

    args = [
        values_in, input_state_in, output_state_in, step_in.T, log_decay_extra.T, conv_x, conv_b, conv_c,
        dt_bias.reshape(1, heads), decay_rate.reshape(1, heads),
    ]
    outs = [
        shape((span, inner), BF16), shape((span, shared), BF16), shape((span, shared), BF16), shape((heads, span), F32),
        shape((heads, span), F32), shape((STATE, inner), F32), shape((EXTRA, inner), BF16), shape((EDGE, inner), F32),
        shape((EDGE, inner + 2 * shared), BF16), shape((EDGE, inner + 2 * shared), BF16),
    ]
    x_act, b_act, c_act, cum, step, state, logs, edge_weight, head, tail = pl.pallas_call(
        local_kernel,
        out_shape=outs,
        in_specs=[pl.BlockSpec(memory_space=pltpu.HBM)] * len(args),
        out_specs=whole(len(outs)),
        scratch_shapes=[vmem((span + 8, 256), F32)] + [vmem(a.shape, a.dtype) for a in args] + [pltpu.SemaphoreType.DMA((len(args),))],
        compiler_params=pltpu.CompilerParams(vmem_limit_bytes=LARGE),
        cost_estimate=pl.CostEstimate(flops=FILL, bytes_accessed=4_000_000, transcendentals=0),
        name="local",
    )(*(pltpu.with_memory_space_constraint(a, pltpu.HBM) for a in args))
    halo = move(tail, [(i, i + 1) for i in range(places - 1)])
    payload = shape((STATE + EXTRA, quarter), BF16)
    edge_x, edge_b, edge_c, *slots = local_call(
        edge_kernel,
        [
            shape((EDGE, inner), BF16), shape((EDGE, shared), BF16), shape((EDGE, shared), BF16), payload, payload, payload, payload,
        ],
        [head, halo, conv_x, conv_b, conv_c, state, logs, edge_weight],
        [vmem((2 * EDGE, inner + 2 * shared), F32), vmem((STATE + EXTRA, inner), BF16)],
        limit=SMALL,
    )

    gate, grow = local_call(gate_kernel, [shape((span, inner), F32)] * 2, [gate_in, cum], flops=FILL)
    y_inside, c_all = local_call(
        inside_kernel,
        [shape((span, inner), F32), shape((span, shared), BF16)],
        [x_act, b_act, c_act, edge_x, edge_b, edge_c, cum, step, gate],
        [
            vmem((span, shared), BF16), vmem((BLOCK, inner), BF16), vmem((BLOCK, BLOCK), F32), vmem((BLOCK, BLOCK), F32),
            vmem((STATE, inner), F32),
        ],
        flops=FILL,
    )

    order = vmem((QUAD, STATE + EXTRA, quarter), BF16)
    arrived = {bits: exchange(slots[bits], bits) for bits in (3, 2, 1)}
    quad = [slots[0], arrived[1], arrived[2], arrived[3]]
    slice_of = shape((STATE, quarter), BF16)
    kept = [shape((STATE, quarter), F32), shape((1, quarter), F32)]
    first, sent, total, log = local_call(quad_total_kernel, [slice_of, payload, *kept], quad, [order], limit=SMALL)
    fours = places // QUAD
    half = fours // 2

    def up(x, sources, distance):
        return move(x, [(i, i + distance * QUAD) for four in sources for i in range(four * QUAD, (four + 1) * QUAD)])

    def jump(four, before, last=None):
        if last is None:
            kernel = lambda *refs: jump_kernel(four, refs[0], None, *refs[1:])
            return local_call(kernel, slice_of, [before, total, log], limit=SMALL)
        return local_call(functools.partial(jump_kernel, four), slice_of, [before, last, total, log], limit=SMALL)

    pairs = up(sent, range(half, fours, 2), 1)
    arrived, targets = [], []

    def send(x, four, distance):
        arrived.append(up(x, (four,), distance))
        targets.append(four + distance)
        return arrived[-1]

    before = send(first, 0, 1)
    for four in range(1, half - 1):
        before = send(jump(four, before), four, 1)
    senders, values = list(range(half - 1, fours - 1, 2)), []
    for four in senders:
        values.append(jump(four, before, pairs if values else None))
        before = send(values[-1], four, 2)
    chosen = local_call(functools.partial(choose_kernel, tuple(senders)), slice_of, values, limit=SMALL)
    side = up(chosen, senders, 1)
    for four in senders:
        arrived.append(side)
        targets.append(four + 1)
    ends = local_call(
        functools.partial(prefix_kernel, tuple(targets)),
        [slice_of] * QUAD,
        [*arrived, pairs, *quad],
        [order, vmem((QUAD, STATE, quarter), BF16), vmem(payload.shape, BF16), vmem(slice_of.shape, BF16)],
        limit=SMALL,
    )
    carried = {bits: exchange(ends[bits], bits) for bits in (3, 2, 1)}

    def projected(own):
        return local_call(
            functools.partial(output_kernel, own),
            shape((span // 2, w_out.shape[1]), F32 if own else BF16),
            [y_inside, grow, c_all, out_gain.reshape(1, inner), ends[0], carried[1], carried[2], carried[3], w_out],
            [vmem((STATE, inner), BF16), vmem((span // 2, inner), BF16)],
            flops=FILL,
        )

    theirs = projected(False)
    other = lax.ppermute(theirs, "tp", [(0, 1), (1, 0)])
    mine = projected(True)
    return local_call(sum_kernel, shape(mine.shape, BF16), [mine, other])


def solution(mesh):
    rows = P(("grp", "sp"), "tp")
    placed = (rows, rows, rows, rows, rows, P(None, "tp"), P(None, "tp"), P(None, "tp"), P("tp"), P("tp"), rows, P("tp"), P("tp", None))
    return jax.shard_map(body, mesh=mesh, in_specs=placed, out_specs=P(("grp", "sp", "tp"), None), check_vma=False)
```

```python
import functools

import jax
import jax.numpy as jnp
from jax import lax
from jax.experimental import pallas as pl
from jax.experimental.pallas import tpu as pltpu
from jax.sharding import PartitionSpec as P


HEAD_DIM = 64
STATE = 128
CONV = 4
BLOCK = 128
QUAD = 4
EXTRA = 16
EPS = 1e-05
F32 = jnp.float32
BF16 = jnp.bfloat16
EDGE = 16
FILL = 4_000_000_000
SMALL = 4 * 1024 * 1024
LARGE = 16 * 1024 * 1024


def dot(a, b, dims=((1,), (0,))):
    return lax.dot_general(a, b, (dims, ((), ())), preferred_element_type=F32)


def parts_of(x, count):
    out = []
    for _ in range(count):
        part = x.astype(BF16)
        out.append(part)
        x = x - part.astype(F32)
    return out


def spread_matrix(heads):
    row = lax.broadcasted_iota(jnp.int32, (heads, heads * HEAD_DIM), 0)
    col = lax.broadcasted_iota(jnp.int32, (heads, heads * HEAD_DIM), 1)
    return (row == col // HEAD_DIM).astype(F32).astype(BF16)


def spread(x, matrix, count=2):
    return dot(jnp.concatenate(parts_of(x, count), axis=0), jnp.concatenate([matrix] * count, axis=0), ((0,), (0,)))


def column(row):
    size = row.shape[1]
    same = lax.broadcasted_iota(jnp.int32, (size, size), 0) == lax.broadcasted_iota(jnp.int32, (size, size), 1)
    return jnp.sum(jnp.where(same, row, 0.0), axis=1, keepdims=True)


def softplus(x):
    return jnp.maximum(x, 0.0) + jnp.log1p(jnp.exp(-jnp.abs(x)))


def silu(x):
    half = 0.5 * x
    return half + half * jnp.tanh(half)


def convolved(ext, first, rows, taps):
    summed = jnp.zeros((rows, ext.shape[1]), F32)
    for tap in range(CONV):
        summed = summed + taps[tap : tap + 1].astype(F32) * ext[first + tap : first + tap + rows, :]
    return silu(summed).astype(BF16)


def local_kernel(
    values_hbm, b_hbm, c_hbm, step_hbm, extra_hbm, conv_x_hbm, conv_b_hbm, conv_c_hbm, dt_hbm, rate_hbm,
    x_act, b_act, c_act, cum_out, step_out, state_out, logs_out, edge_weight, head,
    ext, values, b_in, c_in, step_in, extra, conv_x, conv_b, conv_c, dt_bias, rate, sems,
):
    sources = (step_hbm, extra_hbm, dt_hbm, rate_hbm, b_hbm, conv_b_hbm, c_hbm, conv_c_hbm, values_hbm, conv_x_hbm)
    targets = (step_in, extra, dt_bias, rate, b_in, conv_b, c_in, conv_c, values, conv_x)
    copies = [pltpu.make_async_copy(source, target, sems.at[turn]) for turn, (source, target) in enumerate(zip(sources, targets, strict=True))]
    for copy in copies:
        copy.start()
    for copy in copies[:4]:
        copy.wait()
    span, inner = values.shape
    heads = step_in.shape[0]
    step = softplus(step_in[...].astype(F32) + column(dt_bias[...]))
    log_step = extra[...] - step * column(rate[...])
    step_out[...] = step
    row = lax.broadcasted_iota(jnp.int32, (BLOCK, BLOCK), 0)
    upper = (row <= lax.broadcasted_iota(jnp.int32, (BLOCK, BLOCK), 1)).astype(F32).astype(BF16)
    total = jnp.zeros((heads, 1), F32)
    for start in range(0, span, BLOCK):
        summed = dot(jnp.concatenate(parts_of(log_step[:, start : start + BLOCK], 3), axis=0), upper)
        cum = summed[:heads] + summed[heads : 2 * heads] + summed[2 * heads :] + total
        cum_out[:, start : start + BLOCK] = cum
        total = cum[:, BLOCK - 1 :]
    matrix = spread_matrix(heads)
    weight = jnp.exp(total - cum_out[...]) * step
    edge_weight[...] = spread(weight[:, 0:BLOCK], matrix)[0:EDGE]
    lane = lax.broadcasted_iota(jnp.int32, (heads, BLOCK), 1)
    high, middle, low = (part.astype(F32) for part in parts_of(total, 3))
    logs = jnp.where(lane == 0, high, jnp.where(lane == 1, middle, jnp.where(lane == 2, low, 0.0)))
    logs_out[...] = dot(logs.astype(BF16), matrix, ((0,), (0,)))[0:EXTRA].astype(BF16)
    weight = jnp.where(lax.broadcasted_iota(jnp.int32, (heads, span), 1) < EDGE, 0.0, weight)
    width = ext.shape[1]
    ext[0:8, :] = jnp.zeros((8, width), F32)
    per_group = inner // (b_in.shape[1] // STATE)
    offset = 0
    for turn, (source, taps, target) in enumerate(((b_in, conv_b, b_act), (c_in, conv_c, c_act), (values, conv_x, x_act))):
        for copy in copies[4 + 2 * turn : 6 + 2 * turn]:
            copy.wait()
        head[:, offset : offset + source.shape[1]] = source[0:EDGE, :]
        offset += source.shape[1]
        for start in range(0, source.shape[1], width):
            lanes = slice(start, start + width)
            ext[8 : 8 + span, :] = source[:, lanes].astype(F32)
            active = convolved(ext, 8 - (CONV - 1), span, taps[:, lanes])
            target[:, lanes] = active
            if source is values:
                group = start // per_group
                weighted = (active.astype(F32) * spread(weight, matrix[:, lanes])).astype(BF16)
                state_out[:, lanes] = dot(b_act[:, group * STATE : (group + 1) * STATE], weighted, ((0,), (0,)))


def edge_kernel(
    head, halo, conv_x, conv_b, conv_c, state_in, logs_in, edge_weight,
    edge_x, edge_b, edge_c, slot0, slot1, slot2, slot3, ext, packed,
):
    inner, shared = edge_x.shape[1], edge_b.shape[1]
    ext[0:EDGE, :] = halo[...].astype(F32)
    ext[EDGE : 2 * EDGE, :] = head[...].astype(F32)
    offset = 0
    for taps, target in ((conv_b, edge_b), (conv_c, edge_c), (conv_x, edge_x)):
        lanes = slice(offset, offset + target.shape[1])
        target[...] = convolved(ext.at[:, lanes], EDGE - (CONV - 1), EDGE, taps[...])
        offset += target.shape[1]
    groups = shared // STATE
    weighted = (edge_x[...].astype(F32) * edge_weight[...]).astype(BF16)
    for group in range(groups):
        lanes = slice(group * (inner // groups), (group + 1) * (inner // groups))
        added = dot(edge_b[:, group * STATE : (group + 1) * STATE], weighted[:, lanes], ((0,), (0,)))
        packed[0:STATE, lanes] = (state_in[:, lanes] + added).astype(BF16)
    packed[STATE:, :] = logs_in[...]
    me = lax.rem(lax.axis_index("sp"), QUAD)
    quarter = inner // QUAD
    for bits, slot in enumerate((slot0, slot1, slot2, slot3)):
        slot[...] = packed[:, pl.ds(pl.multiple_of((me ^ bits) * quarter, 128), quarter)]


def whole(count):
    return [pl.BlockSpec(memory_space=pltpu.VMEM)] * count


def local_call(kernel, outs, args, scratch=(), flops=0, limit=None):
    many = isinstance(outs, (list, tuple))
    size = sum(a.size * a.dtype.itemsize for a in args)
    return pl.pallas_call(
        kernel,
        out_shape=outs,
        in_specs=whole(len(args)),
        out_specs=whole(len(outs)) if many else whole(1)[0],
        scratch_shapes=list(scratch),
        compiler_params=pltpu.CompilerParams(vmem_limit_bytes=limit or LARGE),
        cost_estimate=pl.CostEstimate(flops=flops, bytes_accessed=size, transcendentals=0),
    )(*args)


def load(ref):
    logs = ref[STATE:, :].astype(F32)
    return ref[0:STATE, :].astype(F32), logs[0:1] + logs[1:2] + logs[2:3]


def quad_order(ordered, refs):
    me = lax.rem(lax.axis_index("sp"), QUAD)
    for bits, ref in enumerate(refs):
        ordered[me ^ bits] = ref[...]


def store(ref, state, log):
    ref[0:STATE, :] = state.astype(BF16)
    high, middle, low = (part.astype(F32) for part in parts_of(log, 3))
    row = lax.broadcasted_iota(jnp.int32, (EXTRA, log.shape[1]), 0)
    logs = jnp.where(row == 0, high, jnp.where(row == 1, middle, jnp.where(row == 2, low, 0.0)))
    ref[STATE:, :] = logs.astype(BF16)


def quad_total_kernel(own, r1, r2, r3, first, sent, state_out, log_out, ordered):
    quad_order(ordered, (own, r1, r2, r3))
    state, log = load(ordered.at[0])
    for place in range(1, QUAD):
        part, part_log = load(ordered.at[place])
        state, log = state * jnp.exp(part_log) + part, log + part_log
    first[...] = state.astype(BF16)
    store(sent, state, log)
    state_out[...] = state
    log_out[...] = log


def jump_kernel(four, before, last, total, total_log, out):
    @pl.when(lax.axis_index("sp") // QUAD == four)
    def _():
        state = before[0:STATE, :].astype(F32)
        if last is not None:
            part, log = load(last)
            state = state * jnp.exp(log) + part
        out[...] = (state * jnp.exp(total_log[...]) + total[...]).astype(BF16)


def choose_kernel(fours, *refs):
    for four, ref in zip(fours, refs, strict=False):

        @pl.when(lax.axis_index("sp") // QUAD == four)
        def _(ref=ref):
            refs[-1][...] = ref[...]


def prefix_kernel(targets, *refs):
    ordered, ends, held, got = refs[-4:]
    quad, outs = refs[-12:-8], refs[-8:-4]
    arrived, pairs = refs[:-13], refs[-13]
    place = lax.axis_index("sp")
    group = place // QUAD
    quad_order(ordered, quad)
    held[...] = jnp.zeros_like(held)
    got[...] = jnp.zeros_like(got)
    for target, ref in zip(targets, arrived, strict=True):

        @pl.when(group == target)
        def _(ref=ref):
            got[...] = ref[0:STATE, :]

    @pl.when(jnp.logical_and(group > max(targets) // 2, lax.rem(group, 2) == 1))
    def _():
        held[...] = pairs[...]

    state, log = load(held)
    state = got[...].astype(F32) * jnp.exp(log) + state
    ends[0] = state.astype(BF16)
    for turn in range(QUAD - 1):
        part, log = load(ordered.at[turn])
        state = state * jnp.exp(log) + part
        ends[turn + 1] = state.astype(BF16)
    me = lax.rem(place, QUAD)
    for bits, out in enumerate(outs):
        out[...] = ends[me ^ bits]


def gate_kernel(gate, cum_all, gate_out, grow_out):
    matrix = spread_matrix(cum_all.shape[0])
    width = 256
    grow = jnp.exp(cum_all[...])
    for start in range(0, gate.shape[1], width):
        lanes = slice(start, start + width)
        gated = silu(gate[:, lanes].astype(F32))
        gate_out[:, lanes] = gated
        grow_out[:, lanes] = gated * spread(grow, matrix[:, lanes])


def inside_kernel(
    x_act, b_act, c_act, edge_x, edge_b, edge_c, cum_all, step_all, gate,
    y_out, c_out, b_all, x_first, padded, turned, entering,
):
    span, _ = x_act.shape
    heads = step_all.shape[0]
    groups = b_act.shape[1] // STATE
    per_group = heads // groups
    matrix = spread_matrix(heads)
    keep = lax.broadcasted_iota(jnp.int32, (BLOCK, BLOCK), 0) >= lax.broadcasted_iota(jnp.int32, (BLOCK, BLOCK), 1)
    left = lax.broadcasted_iota(jnp.int32, (BLOCK, 2 * HEAD_DIM), 1) < HEAD_DIM
    c_out[...] = c_act[...]
    c_out[0:EDGE, :] = edge_c[...]
    b_all[...] = b_act[...]
    b_all[0:EDGE, :] = edge_b[...]
    x_first[...] = x_act[0:BLOCK, :]
    x_first[0:EDGE, :] = edge_x[...]
    padded[...] = jnp.zeros_like(padded)
    before = jnp.zeros((heads, 1), F32)
    for start in range(0, span, BLOCK):
        rows = slice(start, start + BLOCK)
        x_blk = x_first if start == 0 else x_act.at[rows]
        cum = cum_all[:, rows] - before
        step = step_all[:, rows]
        padded[0:heads, :] = cum
        turned[...] = jnp.transpose(padded[...])
        total = cum[:, BLOCK - 1 :]
        before = before + total
        grow = jnp.exp(cum)
        weight = jnp.exp(total - cum) * step
        for group in range(groups):
            lanes = slice(group * STATE, (group + 1) * STATE)
            channels = slice(group * per_group * HEAD_DIM, (group + 1) * per_group * HEAD_DIM)
            b_blk, c_blk = b_all[rows, lanes], c_out[rows, lanes]
            scores = dot(c_blk, b_blk, ((1,), (1,)))
            if start > 0:
                read = dot(c_blk, entering[:, channels].astype(BF16)) * spread(grow, matrix[:, channels])
            for pair in range(per_group // 2):
                first = (group * per_group + 2 * pair) * HEAD_DIM
                results = []
                for head in (group * per_group + 2 * pair, group * per_group + 2 * pair + 1):
                    difference = turned[:, head : head + 1] - cum[head : head + 1, :]
                    decay = jnp.exp(jnp.where(keep, difference, -jnp.inf))
                    mixing = (scores * decay * step[head : head + 1, :]).astype(BF16)
                    results.append(dot(mixing, x_blk[:, first : first + 2 * HEAD_DIM]))
                y = jnp.where(left, results[0], results[1])
                if start > 0:
                    y = y + read[:, 2 * pair * HEAD_DIM : 2 * (pair + 1) * HEAD_DIM]
                y_out[rows, first : first + 2 * HEAD_DIM] = y * gate[rows, first : first + 2 * HEAD_DIM]
            if start + BLOCK < span:
                weighted = (x_blk[:, channels].astype(F32) * spread(weight, matrix[:, channels])).astype(BF16)
                added = dot(b_blk, weighted, ((0,), (0,)))
                if start > 0:
                    grown = spread(jnp.broadcast_to(jnp.exp(total), (heads, BLOCK)), matrix[:, channels], 3)
                    added = entering[:, channels] * grown + added
                entering[:, channels] = added


def output_kernel(own, y_in, grow, c_all, gain, p0, p1, p2, p3, w_out, out, ends, normalized):
    span, inner = y_in.shape
    groups = c_all.shape[1] // STATE
    quarter = inner // QUAD
    half = span // 2
    core = lax.axis_index("tp")
    rows = pl.ds(pl.multiple_of((core if own else 1 - core) * half, 64), half)
    me = lax.rem(lax.axis_index("sp"), QUAD)
    for bits, ref in enumerate((p0, p1, p2, p3)):
        ends[:, pl.ds(pl.multiple_of((me ^ bits) * quarter, 128), quarter)] = ref[...]
    place = lax.broadcasted_iota(jnp.int32, (quarter, quarter), 0) // HEAD_DIM
    same = place == lax.broadcasted_iota(jnp.int32, (quarter, quarter), 1) // HEAD_DIM
    mean = (same.astype(F32) * (1.0 / HEAD_DIM)).astype(BF16)
    for start in range(0, inner, quarter):
        lanes = slice(start, start + quarter)
        group = start // (inner // groups)
        read = dot(c_all[rows, group * STATE : (group + 1) * STATE], ends[:, lanes])
        gated = y_in[rows, lanes] + read * grow[rows, lanes]
        square = sum(dot(part, mean) for part in parts_of(gated * gated, 2))
        normalized[:, lanes] = (gated * lax.rsqrt(square + EPS) * gain[:, lanes].astype(F32)).astype(BF16)
    width = 512
    for start in range(0, w_out.shape[1], width):
        lanes = slice(start, start + width)
        out[:, lanes] = dot(normalized[...], w_out[:, lanes]).astype(out.dtype)


def sum_kernel(own, other, out):
    out[...] = (own[...] + other[...].astype(F32)).astype(BF16)


def tail_kernel(values, b_in, c_in, out, sems):
    offset, copies = 0, []
    for turn, source in enumerate((b_in, c_in, values)):
        rows, lanes = pl.ds(source.shape[0] - EDGE, EDGE), pl.ds(offset, source.shape[1])
        copies.append(pltpu.make_async_copy(source.at[rows, :], out.at[:, lanes], sems.at[turn]))
        offset += source.shape[1]
    for copy in copies:
        copy.start()
    for copy in copies:
        copy.wait()


def body(
    gate_in, values_in, input_state_in, output_state_in, step_in, conv_x, conv_b, conv_c, dt_bias, decay_rate, log_decay_extra,
    out_gain, w_out,
):
    span, inner = values_in.shape
    shared = input_state_in.shape[1]
    heads = step_in.shape[1]
    places = lax.axis_size("sp")
    quarter = inner // QUAD
    shape = jax.ShapeDtypeStruct
    vmem = pltpu.VMEM

    def move(x, route):
        return lax.ppermute(x, "sp", route)

    def exchange(x, bits, count=places):
        return move(x, [(i, i ^ bits) for i in range(count)])

    tail = pl.pallas_call(
        tail_kernel,
        out_shape=shape((EDGE, inner + 2 * shared), BF16),
        in_specs=[pl.BlockSpec(memory_space=pl.ANY)] * 3,
        out_specs=whole(1)[0],
        scratch_shapes=[pltpu.SemaphoreType.DMA((3,))],
        compiler_params=pltpu.CompilerParams(vmem_limit_bytes=SMALL),
        name="tail",
    )(*(pltpu.with_memory_space_constraint(a, pltpu.HBM) for a in (values_in, input_state_in, output_state_in)))
    halo = move(tail, [(i, i + 1) for i in range(places - 1)])
    args = [
        values_in, input_state_in, output_state_in, step_in.T, log_decay_extra.T, conv_x, conv_b, conv_c,
        dt_bias.reshape(1, heads), decay_rate.reshape(1, heads),
    ]
    outs = [
        shape((span, inner), BF16), shape((span, shared), BF16), shape((span, shared), BF16), shape((heads, span), F32),
        shape((heads, span), F32), shape((STATE, inner), F32), shape((EXTRA, inner), BF16), shape((EDGE, inner), F32),
        shape((EDGE, inner + 2 * shared), BF16),
    ]
    x_act, b_act, c_act, cum, step, state, logs, edge_weight, head = pl.pallas_call(
        local_kernel,
        out_shape=outs,
        in_specs=[pl.BlockSpec(memory_space=pltpu.HBM)] * len(args),
        out_specs=whole(len(outs)),
        scratch_shapes=[vmem((span + 8, 256), F32)] + [vmem(a.shape, a.dtype) for a in args] + [pltpu.SemaphoreType.DMA((len(args),))],
        compiler_params=pltpu.CompilerParams(vmem_limit_bytes=LARGE),
        cost_estimate=pl.CostEstimate(flops=FILL, bytes_accessed=4_000_000, transcendentals=0),
        name="local",
    )(*(pltpu.with_memory_space_constraint(a, pltpu.HBM) for a in args))
    payload = shape((STATE + EXTRA, quarter), BF16)
    edge_x, edge_b, edge_c, *slots = local_call(
        edge_kernel,
        [
            shape((EDGE, inner), BF16), shape((EDGE, shared), BF16), shape((EDGE, shared), BF16), payload, payload, payload, payload,
        ],
        [head, halo, conv_x, conv_b, conv_c, state, logs, edge_weight],
        [vmem((2 * EDGE, inner + 2 * shared), F32), vmem((STATE + EXTRA, inner), BF16)],
        limit=SMALL,
    )

    gate, grow = local_call(gate_kernel, [shape((span, inner), F32)] * 2, [gate_in, cum], flops=FILL)
    y_inside, c_all = local_call(
        inside_kernel,
        [shape((span, inner), F32), shape((span, shared), BF16)],
        [x_act, b_act, c_act, edge_x, edge_b, edge_c, cum, step, gate],
        [
            vmem((span, shared), BF16), vmem((BLOCK, inner), BF16), vmem((BLOCK, BLOCK), F32), vmem((BLOCK, BLOCK), F32),
            vmem((STATE, inner), F32),
        ],
        flops=FILL,
    )

    order = vmem((QUAD, STATE + EXTRA, quarter), BF16)
    arrived = {bits: exchange(slots[bits], bits) for bits in (3, 2, 1)}
    quad = [slots[0], arrived[1], arrived[2], arrived[3]]
    slice_of = shape((STATE, quarter), BF16)
    kept = [shape((STATE, quarter), F32), shape((1, quarter), F32)]
    first, sent, total, log = local_call(quad_total_kernel, [slice_of, payload, *kept], quad, [order], limit=SMALL)
    fours = places // QUAD
    half = fours // 2

    def up(x, sources, distance):
        return move(x, [(i, i + distance * QUAD) for four in sources for i in range(four * QUAD, (four + 1) * QUAD)])

    def swap(x, four):
        first, route = four * QUAD, []
        for i in range(places):
            moved = i + QUAD if first <= i < first + QUAD else i - QUAD if first + QUAD <= i < first + 2 * QUAD else i
            route.append((i, moved))
        return move(x, route)

    def jump(four, before, last=None):
        if last is None:
            kernel = lambda *refs: jump_kernel(four, refs[0], None, *refs[1:])
            return local_call(kernel, slice_of, [before, total, log], limit=SMALL)
        return local_call(functools.partial(jump_kernel, four), slice_of, [before, last, total, log], limit=SMALL)

    pairs = up(sent, range(half, fours, 2), 1)
    arrived, targets = [], []

    def send(x, four, distance):
        arrived.append(swap(x, four) if distance == 1 else up(x, (four,), distance))
        targets.append(four + distance)
        return arrived[-1]

    before = send(first, 0, 1)
    for four in range(1, half - 1):
        before = send(jump(four, before), four, 1)
    senders, values = list(range(half - 1, fours - 1, 2)), []
    for four in senders:
        values.append(jump(four, before, pairs if values else None))
        before = send(values[-1], four, 2)
    chosen = local_call(functools.partial(choose_kernel, tuple(senders)), slice_of, values, limit=SMALL)
    side = up(chosen, senders, 1)
    for four in senders:
        arrived.append(side)
        targets.append(four + 1)
    ends = local_call(
        functools.partial(prefix_kernel, tuple(targets)),
        [slice_of] * QUAD,
        [*arrived, pairs, *quad],
        [order, vmem((QUAD, STATE, quarter), BF16), vmem(payload.shape, BF16), vmem(slice_of.shape, BF16)],
        limit=SMALL,
    )
    carried = {bits: exchange(ends[bits], bits) for bits in (3, 2, 1)}

    def projected(own):
        return local_call(
            functools.partial(output_kernel, own),
            shape((span // 2, w_out.shape[1]), F32 if own else BF16),
            [y_inside, grow, c_all, out_gain.reshape(1, inner), ends[0], carried[1], carried[2], carried[3], w_out],
            [vmem((STATE, inner), BF16), vmem((span // 2, inner), BF16)],
            flops=FILL,
        )

    theirs = projected(False)
    other = lax.ppermute(theirs, "tp", [(0, 1), (1, 0)])
    mine = projected(True)
    return local_call(sum_kernel, shape(mine.shape, BF16), [mine, other])


def solution(mesh):
    rows = P(("grp", "sp"), "tp")
    placed = (rows, rows, rows, rows, rows, P(None, "tp"), P(None, "tp"), P(None, "tp"), P("tp"), P("tp"), rows, P("tp"), P("tp", None))
    return jax.shard_map(body, mesh=mesh, in_specs=placed, out_specs=P(("grp", "sp", "tp"), None), check_vma=False)
```

```python
import functools

import jax
import jax.numpy as jnp
from jax import lax
from jax.experimental import pallas as pl
from jax.experimental.pallas import tpu as pltpu
from jax.sharding import PartitionSpec as P


HEAD_DIM = 64
STATE = 128
CONV = 4
BLOCK = 128
QUAD = 4
EXTRA = 16
EPS = 1e-05
F32 = jnp.float32
BF16 = jnp.bfloat16
EDGE = 16
FILL = 4_000_000_000
SMALL = 4 * 1024 * 1024
LARGE = 16 * 1024 * 1024


def dot(a, b, dims=((1,), (0,))):
    return lax.dot_general(a, b, (dims, ((), ())), preferred_element_type=F32)


def parts_of(x, count):
    out = []
    for _ in range(count):
        part = x.astype(BF16)
        out.append(part)
        x = x - part.astype(F32)
    return out


def spread_matrix(heads):
    row = lax.broadcasted_iota(jnp.int32, (heads, heads * HEAD_DIM), 0)
    col = lax.broadcasted_iota(jnp.int32, (heads, heads * HEAD_DIM), 1)
    return (row == col // HEAD_DIM).astype(F32).astype(BF16)


def spread(x, matrix, count=2):
    return dot(jnp.concatenate(parts_of(x, count), axis=0), jnp.concatenate([matrix] * count, axis=0), ((0,), (0,)))


def column(row):
    size = row.shape[1]
    same = lax.broadcasted_iota(jnp.int32, (size, size), 0) == lax.broadcasted_iota(jnp.int32, (size, size), 1)
    return jnp.sum(jnp.where(same, row, 0.0), axis=1, keepdims=True)


def softplus(x):
    return jnp.maximum(x, 0.0) + jnp.log1p(jnp.exp(-jnp.abs(x)))


def silu(x):
    half = 0.5 * x
    return half + half * jnp.tanh(half)


def convolved(ext, first, rows, taps):
    summed = jnp.zeros((rows, ext.shape[1]), F32)
    for tap in range(CONV):
        summed = summed + taps[tap : tap + 1].astype(F32) * ext[first + tap : first + tap + rows, :]
    return silu(summed).astype(BF16)


def local_kernel(
    values_hbm, b_hbm, c_hbm, step_hbm, extra_hbm, conv_x_hbm, conv_b_hbm, conv_c_hbm, dt_hbm, rate_hbm,
    x_act, b_act, c_act, cum_out, step_out, state_out, logs_out, edge_weight, head,
    ext, values, b_in, c_in, step_in, extra, conv_x, conv_b, conv_c, dt_bias, rate, sems,
):
    sources = (step_hbm, extra_hbm, dt_hbm, rate_hbm, b_hbm, conv_b_hbm, c_hbm, conv_c_hbm, values_hbm, conv_x_hbm)
    targets = (step_in, extra, dt_bias, rate, b_in, conv_b, c_in, conv_c, values, conv_x)
    copies = [pltpu.make_async_copy(source, target, sems.at[turn]) for turn, (source, target) in enumerate(zip(sources, targets, strict=True))]
    for copy in copies:
        copy.start()
    for copy in copies[:4]:
        copy.wait()
    span, inner = values.shape
    heads = step_in.shape[0]
    step = softplus(step_in[...].astype(F32) + column(dt_bias[...]))
    log_step = extra[...] - step * column(rate[...])
    step_out[...] = step
    row = lax.broadcasted_iota(jnp.int32, (BLOCK, BLOCK), 0)
    upper = (row <= lax.broadcasted_iota(jnp.int32, (BLOCK, BLOCK), 1)).astype(F32).astype(BF16)
    total = jnp.zeros((heads, 1), F32)
    for start in range(0, span, BLOCK):
        summed = dot(jnp.concatenate(parts_of(log_step[:, start : start + BLOCK], 3), axis=0), upper)
        cum = summed[:heads] + summed[heads : 2 * heads] + summed[2 * heads :] + total
        cum_out[:, start : start + BLOCK] = cum
        total = cum[:, BLOCK - 1 :]
    matrix = spread_matrix(heads)
    weight = jnp.exp(total - cum_out[...]) * step
    edge_weight[...] = spread(weight[:, 0:BLOCK], matrix)[0:EDGE]
    lane = lax.broadcasted_iota(jnp.int32, (heads, BLOCK), 1)
    high, middle, low = (part.astype(F32) for part in parts_of(total, 3))
    logs = jnp.where(lane == 0, high, jnp.where(lane == 1, middle, jnp.where(lane == 2, low, 0.0)))
    logs_out[...] = dot(logs.astype(BF16), matrix, ((0,), (0,)))[0:EXTRA].astype(BF16)
    weight = jnp.where(lax.broadcasted_iota(jnp.int32, (heads, span), 1) < EDGE, 0.0, weight)
    width = ext.shape[1]
    ext[0:8, :] = jnp.zeros((8, width), F32)
    per_group = inner // (b_in.shape[1] // STATE)
    offset = 0
    for turn, (source, taps, target) in enumerate(((b_in, conv_b, b_act), (c_in, conv_c, c_act), (values, conv_x, x_act))):
        for copy in copies[4 + 2 * turn : 6 + 2 * turn]:
            copy.wait()
        head[:, offset : offset + source.shape[1]] = source[0:EDGE, :]
        offset += source.shape[1]
        for start in range(0, source.shape[1], width):
            lanes = slice(start, start + width)
            ext[8 : 8 + span, :] = source[:, lanes].astype(F32)
            active = convolved(ext, 8 - (CONV - 1), span, taps[:, lanes])
            target[:, lanes] = active
            if source is values:
                group = start // per_group
                weighted = (active.astype(F32) * spread(weight, matrix[:, lanes])).astype(BF16)
                state_out[:, lanes] = dot(b_act[:, group * STATE : (group + 1) * STATE], weighted, ((0,), (0,)))


def edge_kernel(
    head, halo, conv_x, conv_b, conv_c, state_in, logs_in, edge_weight,
    edge_x, edge_b, edge_c, slot0, slot1, slot2, slot3, ext, packed,
):
    inner, shared = edge_x.shape[1], edge_b.shape[1]
    ext[0:EDGE, :] = halo[...].astype(F32)
    ext[EDGE : 2 * EDGE, :] = head[...].astype(F32)
    offset = 0
    for taps, target in ((conv_b, edge_b), (conv_c, edge_c), (conv_x, edge_x)):
        lanes = slice(offset, offset + target.shape[1])
        target[...] = convolved(ext.at[:, lanes], EDGE - (CONV - 1), EDGE, taps[...])
        offset += target.shape[1]
    groups = shared // STATE
    weighted = (edge_x[...].astype(F32) * edge_weight[...]).astype(BF16)
    for group in range(groups):
        lanes = slice(group * (inner // groups), (group + 1) * (inner // groups))
        added = dot(edge_b[:, group * STATE : (group + 1) * STATE], weighted[:, lanes], ((0,), (0,)))
        packed[0:STATE, lanes] = (state_in[:, lanes] + added).astype(BF16)
    packed[STATE:, :] = logs_in[...]
    me = lax.rem(lax.axis_index("sp"), QUAD)
    quarter = inner // QUAD
    for bits, slot in enumerate((slot0, slot1, slot2, slot3)):
        slot[...] = packed[:, pl.ds(pl.multiple_of((me ^ bits) * quarter, 128), quarter)]


def whole(count):
    return [pl.BlockSpec(memory_space=pltpu.VMEM)] * count


def local_call(kernel, outs, args, scratch=(), flops=0, limit=None):
    many = isinstance(outs, (list, tuple))
    size = sum(a.size * a.dtype.itemsize for a in args)
    return pl.pallas_call(
        kernel,
        out_shape=outs,
        in_specs=whole(len(args)),
        out_specs=whole(len(outs)) if many else whole(1)[0],
        scratch_shapes=list(scratch),
        compiler_params=pltpu.CompilerParams(vmem_limit_bytes=limit or LARGE),
        cost_estimate=pl.CostEstimate(flops=flops, bytes_accessed=size, transcendentals=0),
    )(*args)


def load(ref):
    logs = ref[STATE:, :].astype(F32)
    return ref[0:STATE, :].astype(F32), logs[0:1] + logs[1:2] + logs[2:3]


def quad_order(ordered, refs):
    me = lax.rem(lax.axis_index("sp"), QUAD)
    for bits, ref in enumerate(refs):
        ordered[me ^ bits] = ref[...]


def store(ref, state, log):
    ref[0:STATE, :] = state.astype(BF16)
    high, middle, low = (part.astype(F32) for part in parts_of(log, 3))
    row = lax.broadcasted_iota(jnp.int32, (EXTRA, log.shape[1]), 0)
    logs = jnp.where(row == 0, high, jnp.where(row == 1, middle, jnp.where(row == 2, low, 0.0)))
    ref[STATE:, :] = logs.astype(BF16)


def quad_total_kernel(own, r1, r2, r3, first, sent, state_out, log_out, ordered):
    quad_order(ordered, (own, r1, r2, r3))
    state, log = load(ordered.at[0])
    for place in range(1, QUAD):
        part, part_log = load(ordered.at[place])
        state, log = state * jnp.exp(part_log) + part, log + part_log
    first[...] = state.astype(BF16)
    store(sent, state, log)
    state_out[...] = state
    log_out[...] = log


def jump_kernel(four, before, last, total, total_log, out):
    @pl.when(lax.axis_index("sp") // QUAD == four)
    def _():
        state = before[0:STATE, :].astype(F32)
        if last is not None:
            part, log = load(last)
            state = state * jnp.exp(log) + part
        out[...] = (state * jnp.exp(total_log[...]) + total[...]).astype(BF16)


def choose_kernel(fours, *refs):
    for four, ref in zip(fours, refs, strict=False):

        @pl.when(lax.axis_index("sp") // QUAD == four)
        def _(ref=ref):
            refs[-1][...] = ref[...]


def prefix_kernel(targets, *refs):
    ordered, ends, held, got = refs[-4:]
    quad, outs = refs[-12:-8], refs[-8:-4]
    arrived, pairs = refs[:-13], refs[-13]
    place = lax.axis_index("sp")
    group = place // QUAD
    quad_order(ordered, quad)
    held[...] = jnp.zeros_like(held)
    got[...] = jnp.zeros_like(got)
    for target, ref in zip(targets, arrived, strict=True):

        @pl.when(group == target)
        def _(ref=ref):
            got[...] = ref[0:STATE, :]

    @pl.when(jnp.logical_and(group > max(targets) // 2, lax.rem(group, 2) == 1))
    def _():
        held[...] = pairs[...]

    state, log = load(held)
    state = got[...].astype(F32) * jnp.exp(log) + state
    ends[0] = state.astype(BF16)
    for turn in range(QUAD - 1):
        part, log = load(ordered.at[turn])
        state = state * jnp.exp(log) + part
        ends[turn + 1] = state.astype(BF16)
    me = lax.rem(place, QUAD)
    for bits, out in enumerate(outs):
        out[...] = ends[me ^ bits]


def gate_kernel(gate, cum_all, gate_out, grow_out):
    matrix = spread_matrix(cum_all.shape[0])
    width = 256
    grow = jnp.exp(cum_all[...])
    for start in range(0, gate.shape[1], width):
        lanes = slice(start, start + width)
        gated = silu(gate[:, lanes].astype(F32))
        gate_out[:, lanes] = gated
        grow_out[:, lanes] = gated * spread(grow, matrix[:, lanes])


def inside_kernel(
    x_act, b_act, c_act, edge_x, edge_b, edge_c, cum_all, step_all, gate,
    y_out, c_out, b_all, x_first, padded, turned, entering,
):
    span, _ = x_act.shape
    heads = step_all.shape[0]
    groups = b_act.shape[1] // STATE
    per_group = heads // groups
    matrix = spread_matrix(heads)
    keep = lax.broadcasted_iota(jnp.int32, (BLOCK, BLOCK), 0) >= lax.broadcasted_iota(jnp.int32, (BLOCK, BLOCK), 1)
    left = lax.broadcasted_iota(jnp.int32, (BLOCK, 2 * HEAD_DIM), 1) < HEAD_DIM
    c_out[...] = c_act[...]
    c_out[0:EDGE, :] = edge_c[...]
    b_all[...] = b_act[...]
    b_all[0:EDGE, :] = edge_b[...]
    x_first[...] = x_act[0:BLOCK, :]
    x_first[0:EDGE, :] = edge_x[...]
    padded[...] = jnp.zeros_like(padded)
    before = jnp.zeros((heads, 1), F32)
    for start in range(0, span, BLOCK):
        rows = slice(start, start + BLOCK)
        x_blk = x_first if start == 0 else x_act.at[rows]
        cum = cum_all[:, rows] - before
        step = step_all[:, rows]
        padded[0:heads, :] = cum
        turned[...] = jnp.transpose(padded[...])
        total = cum[:, BLOCK - 1 :]
        before = before + total
        grow = jnp.exp(cum)
        weight = jnp.exp(total - cum) * step
        for group in range(groups):
            lanes = slice(group * STATE, (group + 1) * STATE)
            channels = slice(group * per_group * HEAD_DIM, (group + 1) * per_group * HEAD_DIM)
            b_blk, c_blk = b_all[rows, lanes], c_out[rows, lanes]
            scores = dot(c_blk, b_blk, ((1,), (1,)))
            if start > 0:
                read = dot(c_blk, entering[:, channels].astype(BF16)) * spread(grow, matrix[:, channels])
            for pair in range(per_group // 2):
                first = (group * per_group + 2 * pair) * HEAD_DIM
                results = []
                for head in (group * per_group + 2 * pair, group * per_group + 2 * pair + 1):
                    difference = turned[:, head : head + 1] - cum[head : head + 1, :]
                    decay = jnp.exp(jnp.where(keep, difference, -jnp.inf))
                    mixing = (scores * decay * step[head : head + 1, :]).astype(BF16)
                    results.append(dot(mixing, x_blk[:, first : first + 2 * HEAD_DIM]))
                y = jnp.where(left, results[0], results[1])
                if start > 0:
                    y = y + read[:, 2 * pair * HEAD_DIM : 2 * (pair + 1) * HEAD_DIM]
                y_out[rows, first : first + 2 * HEAD_DIM] = y * gate[rows, first : first + 2 * HEAD_DIM]
            if start + BLOCK < span:
                weighted = (x_blk[:, channels].astype(F32) * spread(weight, matrix[:, channels])).astype(BF16)
                added = dot(b_blk, weighted, ((0,), (0,)))
                if start > 0:
                    grown = spread(jnp.broadcast_to(jnp.exp(total), (heads, BLOCK)), matrix[:, channels], 3)
                    added = entering[:, channels] * grown + added
                entering[:, channels] = added


def output_kernel(own, y_in, grow, c_all, gain, p0, p1, p2, p3, w_out, out, ends, normalized):
    span, inner = y_in.shape
    groups = c_all.shape[1] // STATE
    quarter = inner // QUAD
    half = span // 2
    core = lax.axis_index("tp")
    rows = pl.ds(pl.multiple_of((core if own else 1 - core) * half, 64), half)
    me = lax.rem(lax.axis_index("sp"), QUAD)
    for bits, ref in enumerate((p0, p1, p2, p3)):
        ends[:, pl.ds(pl.multiple_of((me ^ bits) * quarter, 128), quarter)] = ref[...]
    place = lax.broadcasted_iota(jnp.int32, (quarter, quarter), 0) // HEAD_DIM
    same = place == lax.broadcasted_iota(jnp.int32, (quarter, quarter), 1) // HEAD_DIM
    mean = (same.astype(F32) * (1.0 / HEAD_DIM)).astype(BF16)
    for start in range(0, inner, quarter):
        lanes = slice(start, start + quarter)
        group = start // (inner // groups)
        read = dot(c_all[rows, group * STATE : (group + 1) * STATE], ends[:, lanes])
        gated = y_in[rows, lanes] + read * grow[rows, lanes]
        square = sum(dot(part, mean) for part in parts_of(gated * gated, 2))
        normalized[:, lanes] = (gated * lax.rsqrt(square + EPS) * gain[:, lanes].astype(F32)).astype(BF16)
    width = 512
    for start in range(0, w_out.shape[1], width):
        lanes = slice(start, start + width)
        out[:, lanes] = dot(normalized[...], w_out[:, lanes]).astype(out.dtype)


def sum_kernel(own, other, out):
    out[...] = (own[...] + other[...].astype(F32)).astype(BF16)


def tail_kernel(values, b_in, c_in, out, sems):
    offset, copies = 0, []
    for turn, source in enumerate((b_in, c_in, values)):
        rows, lanes = pl.ds(source.shape[0] - EDGE, EDGE), pl.ds(offset, source.shape[1])
        copies.append(pltpu.make_async_copy(source.at[rows, :], out.at[:, lanes], sems.at[turn]))
        offset += source.shape[1]
    for copy in copies:
        copy.start()
    for copy in copies:
        copy.wait()


def body(
    gate_in, values_in, input_state_in, output_state_in, step_in, conv_x, conv_b, conv_c, dt_bias, decay_rate, log_decay_extra,
    out_gain, w_out,
):
    span, inner = values_in.shape
    shared = input_state_in.shape[1]
    heads = step_in.shape[1]
    places = lax.axis_size("sp")
    quarter = inner // QUAD
    shape = jax.ShapeDtypeStruct
    vmem = pltpu.VMEM

    def move(x, route):
        return lax.ppermute(x, "sp", route)

    def exchange(x, bits, count=places):
        return move(x, [(i, i ^ bits) for i in range(count)])

    tail = pl.pallas_call(
        tail_kernel,
        out_shape=shape((EDGE, inner + 2 * shared), BF16),
        in_specs=[pl.BlockSpec(memory_space=pl.ANY)] * 3,
        out_specs=whole(1)[0],
        scratch_shapes=[pltpu.SemaphoreType.DMA((3,))],
        compiler_params=pltpu.CompilerParams(vmem_limit_bytes=SMALL),
        name="tail",
    )(*(pltpu.with_memory_space_constraint(a, pltpu.HBM) for a in (values_in, input_state_in, output_state_in)))
    halo = move(tail, [(i, i + 1) for i in range(places - 1)])
    args = [
        values_in, input_state_in, output_state_in, step_in.T, log_decay_extra.T, conv_x, conv_b, conv_c,
        dt_bias.reshape(1, heads), decay_rate.reshape(1, heads),
    ]
    outs = [
        shape((span, inner), BF16), shape((span, shared), BF16), shape((span, shared), BF16), shape((heads, span), F32),
        shape((heads, span), F32), shape((STATE, inner), F32), shape((EXTRA, inner), BF16), shape((EDGE, inner), F32),
        shape((EDGE, inner + 2 * shared), BF16),
    ]
    x_act, b_act, c_act, cum, step, state, logs, edge_weight, head = pl.pallas_call(
        local_kernel,
        out_shape=outs,
        in_specs=[pl.BlockSpec(memory_space=pltpu.HBM)] * len(args),
        out_specs=whole(len(outs)),
        scratch_shapes=[vmem((span + 8, 256), F32)] + [vmem(a.shape, a.dtype) for a in args] + [pltpu.SemaphoreType.DMA((len(args),))],
        compiler_params=pltpu.CompilerParams(vmem_limit_bytes=LARGE),
        cost_estimate=pl.CostEstimate(flops=FILL, bytes_accessed=4_000_000, transcendentals=0),
        name="local",
    )(*(pltpu.with_memory_space_constraint(a, pltpu.HBM) for a in args))
    payload = shape((STATE + EXTRA, quarter), BF16)
    edge_x, edge_b, edge_c, *slots = local_call(
        edge_kernel,
        [
            shape((EDGE, inner), BF16), shape((EDGE, shared), BF16), shape((EDGE, shared), BF16), payload, payload, payload, payload,
        ],
        [head, halo, conv_x, conv_b, conv_c, state, logs, edge_weight],
        [vmem((2 * EDGE, inner + 2 * shared), F32), vmem((STATE + EXTRA, inner), BF16)],
        limit=SMALL,
    )

    gate, grow = local_call(gate_kernel, [shape((span, inner), F32)] * 2, [gate_in, cum], flops=FILL)
    y_inside, c_all = local_call(
        inside_kernel,
        [shape((span, inner), F32), shape((span, shared), BF16)],
        [x_act, b_act, c_act, edge_x, edge_b, edge_c, cum, step, gate],
        [
            vmem((span, shared), BF16), vmem((BLOCK, inner), BF16), vmem((BLOCK, BLOCK), F32), vmem((BLOCK, BLOCK), F32),
            vmem((STATE, inner), F32),
        ],
        flops=FILL,
    )

    order = vmem((QUAD, STATE + EXTRA, quarter), BF16)
    arrived = {bits: exchange(slots[bits], bits) for bits in (3, 2, 1)}
    quad = [slots[0], arrived[1], arrived[2], arrived[3]]
    slice_of = shape((STATE, quarter), BF16)
    kept = [shape((STATE, quarter), F32), shape((1, quarter), F32)]
    first, sent, total, log = local_call(quad_total_kernel, [slice_of, payload, *kept], quad, [order], limit=SMALL)
    fours = places // QUAD
    half = fours // 2

    def up(x, sources, distance):
        return move(x, [(i, i + distance * QUAD) for four in sources for i in range(four * QUAD, (four + 1) * QUAD)])

    def jump(four, before, last=None):
        if last is None:
            kernel = lambda *refs: jump_kernel(four, refs[0], None, *refs[1:])
            return local_call(kernel, slice_of, [before, total, log], limit=SMALL)
        return local_call(functools.partial(jump_kernel, four), slice_of, [before, last, total, log], limit=SMALL)

    pairs = up(sent, range(half, fours, 2), 1)
    arrived, targets = [], []

    def send(x, four, distance):
        arrived.append(up(x, (four,), distance))
        targets.append(four + distance)
        return arrived[-1]

    before = send(first, 0, 1)
    for four in range(1, half - 1):
        before = send(jump(four, before), four, 1)
    senders, values = list(range(half - 1, fours - 1, 2)), []
    for four in senders:
        values.append(jump(four, before, pairs if values else None))
        before = send(values[-1], four, 2)
    chosen = local_call(functools.partial(choose_kernel, tuple(senders)), slice_of, values, limit=SMALL)
    side = up(chosen, senders, 1)
    for four in senders:
        arrived.append(side)
        targets.append(four + 1)
    ends = local_call(
        functools.partial(prefix_kernel, tuple(targets)),
        [slice_of] * QUAD,
        [*arrived, pairs, *quad],
        [order, vmem((QUAD, STATE, quarter), BF16), vmem(payload.shape, BF16), vmem(slice_of.shape, BF16)],
        limit=SMALL,
    )
    carried = {bits: exchange(ends[bits], bits) for bits in (3, 2, 1)}

    def projected(own):
        return local_call(
            functools.partial(output_kernel, own),
            shape((span // 2, w_out.shape[1]), F32 if own else BF16),
            [y_inside, grow, c_all, out_gain.reshape(1, inner), ends[0], carried[1], carried[2], carried[3], w_out],
            [vmem((STATE, inner), BF16), vmem((span // 2, inner), BF16)],
            flops=FILL,
        )

    theirs = projected(False)
    other = lax.ppermute(theirs, "tp", [(0, 1), (1, 0)])
    mine = projected(True)
    return local_call(sum_kernel, shape(mine.shape, BF16), [mine, other])


def solution(mesh):
    rows = P(("grp", "sp"), "tp")
    placed = (rows, rows, rows, rows, rows, P(None, "tp"), P(None, "tp"), P(None, "tp"), P("tp"), P("tp"), rows, P("tp"), P("tp", None))
    return jax.shard_map(body, mesh=mesh, in_specs=placed, out_specs=P(("grp", "sp", "tp"), None), check_vma=False)
```

```python
import functools

import jax
import jax.numpy as jnp
from jax import lax
from jax.experimental import pallas as pl
from jax.experimental.pallas import tpu as pltpu
from jax.sharding import PartitionSpec as P


HEAD_DIM = 64
STATE = 128
CONV = 4
BLOCK = 128
QUAD = 4
EXTRA = 16
EPS = 1e-05
F32 = jnp.float32
BF16 = jnp.bfloat16
EDGE = 16
FILL = 4_000_000_000
SMALL = 4 * 1024 * 1024
LARGE = 16 * 1024 * 1024


def dot(a, b, dims=((1,), (0,))):
    return lax.dot_general(a, b, (dims, ((), ())), preferred_element_type=F32)


def parts_of(x, count):
    out = []
    for _ in range(count):
        part = x.astype(BF16)
        out.append(part)
        x = x - part.astype(F32)
    return out


def turned_fours(fours):
    half, turned = fours // 2, [False] * fours
    path = [*range(half), *range(half + 1, fours, 2)]
    for turn, four in enumerate(path):
        turned[four] = turn % 2 == 1
        if four >= half - 1 and four + 1 < fours:
            turned[four + 1] = not turned[four]
    return turned


def own_quarter():
    place, fours = lax.axis_index("sp"), lax.axis_size("sp") // QUAD
    mask = sum(1 << four for four, turned in enumerate(turned_fours(fours)) if turned)
    turned = lax.rem(lax.shift_right_logical(jnp.int32(mask), place // QUAD), 2)
    return lax.rem(place, QUAD) ^ ((QUAD - 1) * turned)


def spread_matrix(heads):
    row = lax.broadcasted_iota(jnp.int32, (heads, heads * HEAD_DIM), 0)
    col = lax.broadcasted_iota(jnp.int32, (heads, heads * HEAD_DIM), 1)
    return (row == col // HEAD_DIM).astype(F32).astype(BF16)


def spread(x, matrix, count=2):
    return dot(jnp.concatenate(parts_of(x, count), axis=0), jnp.concatenate([matrix] * count, axis=0), ((0,), (0,)))


def column(row):
    size = row.shape[1]
    same = lax.broadcasted_iota(jnp.int32, (size, size), 0) == lax.broadcasted_iota(jnp.int32, (size, size), 1)
    return jnp.sum(jnp.where(same, row, 0.0), axis=1, keepdims=True)


def softplus(x):
    return jnp.maximum(x, 0.0) + jnp.log1p(jnp.exp(-jnp.abs(x)))


def silu(x):
    half = 0.5 * x
    return half + half * jnp.tanh(half)


def convolved(ext, first, rows, taps):
    summed = jnp.zeros((rows, ext.shape[1]), F32)
    for tap in range(CONV):
        summed = summed + taps[tap : tap + 1].astype(F32) * ext[first + tap : first + tap + rows, :]
    return silu(summed).astype(BF16)


def local_kernel(
    values_hbm, b_hbm, c_hbm, step_hbm, extra_hbm, conv_x_hbm, conv_b_hbm, conv_c_hbm, dt_hbm, rate_hbm,
    x_act, b_act, c_act, cum_out, step_out, state_out, logs_out, edge_weight, head,
    ext, values, b_in, c_in, step_in, extra, conv_x, conv_b, conv_c, dt_bias, rate, sems,
):
    sources = (step_hbm, extra_hbm, dt_hbm, rate_hbm, b_hbm, conv_b_hbm, c_hbm, conv_c_hbm, values_hbm, conv_x_hbm)
    targets = (step_in, extra, dt_bias, rate, b_in, conv_b, c_in, conv_c, values, conv_x)
    copies = [pltpu.make_async_copy(source, target, sems.at[turn]) for turn, (source, target) in enumerate(zip(sources, targets, strict=True))]
    for copy in copies:
        copy.start()
    for copy in copies[:4]:
        copy.wait()
    span, inner = values.shape
    heads = step_in.shape[0]
    step = softplus(step_in[...].astype(F32) + column(dt_bias[...]))
    log_step = extra[...] - step * column(rate[...])
    step_out[...] = step
    row = lax.broadcasted_iota(jnp.int32, (BLOCK, BLOCK), 0)
    upper = (row <= lax.broadcasted_iota(jnp.int32, (BLOCK, BLOCK), 1)).astype(F32).astype(BF16)
    total = jnp.zeros((heads, 1), F32)
    for start in range(0, span, BLOCK):
        summed = dot(jnp.concatenate(parts_of(log_step[:, start : start + BLOCK], 3), axis=0), upper)
        cum = summed[:heads] + summed[heads : 2 * heads] + summed[2 * heads :] + total
        cum_out[:, start : start + BLOCK] = cum
        total = cum[:, BLOCK - 1 :]
    matrix = spread_matrix(heads)
    weight = jnp.exp(total - cum_out[...]) * step
    edge_weight[...] = spread(weight[:, 0:BLOCK], matrix)[0:EDGE]
    lane = lax.broadcasted_iota(jnp.int32, (heads, BLOCK), 1)
    high, middle, low = (part.astype(F32) for part in parts_of(total, 3))
    logs = jnp.where(lane == 0, high, jnp.where(lane == 1, middle, jnp.where(lane == 2, low, 0.0)))
    logs_out[...] = dot(logs.astype(BF16), matrix, ((0,), (0,)))[0:EXTRA].astype(BF16)
    weight = jnp.where(lax.broadcasted_iota(jnp.int32, (heads, span), 1) < EDGE, 0.0, weight)
    width = ext.shape[1]
    ext[0:8, :] = jnp.zeros((8, width), F32)
    per_group = inner // (b_in.shape[1] // STATE)
    offset = 0
    for turn, (source, taps, target) in enumerate(((b_in, conv_b, b_act), (c_in, conv_c, c_act), (values, conv_x, x_act))):
        for copy in copies[4 + 2 * turn : 6 + 2 * turn]:
            copy.wait()
        head[:, offset : offset + source.shape[1]] = source[0:EDGE, :]
        offset += source.shape[1]
        for start in range(0, source.shape[1], width):
            lanes = slice(start, start + width)
            ext[8 : 8 + span, :] = source[:, lanes].astype(F32)
            active = convolved(ext, 8 - (CONV - 1), span, taps[:, lanes])
            target[:, lanes] = active
            if source is values:
                group = start // per_group
                weighted = (active.astype(F32) * spread(weight, matrix[:, lanes])).astype(BF16)
                state_out[:, lanes] = dot(b_act[:, group * STATE : (group + 1) * STATE], weighted, ((0,), (0,)))


def edge_kernel(
    head, halo, conv_x, conv_b, conv_c, state_in, logs_in, edge_weight,
    edge_x, edge_b, edge_c, slot0, slot1, slot2, slot3, ext, packed,
):
    inner, shared = edge_x.shape[1], edge_b.shape[1]
    ext[0:EDGE, :] = halo[...].astype(F32)
    ext[EDGE : 2 * EDGE, :] = head[...].astype(F32)
    offset = 0
    for taps, target in ((conv_b, edge_b), (conv_c, edge_c), (conv_x, edge_x)):
        lanes = slice(offset, offset + target.shape[1])
        target[...] = convolved(ext.at[:, lanes], EDGE - (CONV - 1), EDGE, taps[...])
        offset += target.shape[1]
    groups = shared // STATE
    weighted = (edge_x[...].astype(F32) * edge_weight[...]).astype(BF16)
    for group in range(groups):
        lanes = slice(group * (inner // groups), (group + 1) * (inner // groups))
        added = dot(edge_b[:, group * STATE : (group + 1) * STATE], weighted[:, lanes], ((0,), (0,)))
        packed[0:STATE, lanes] = (state_in[:, lanes] + added).astype(BF16)
    packed[STATE:, :] = logs_in[...]
    me = own_quarter()
    quarter = inner // QUAD
    for bits, slot in enumerate((slot0, slot1, slot2, slot3)):
        slot[...] = packed[:, pl.ds(pl.multiple_of((me ^ bits) * quarter, 128), quarter)]


def whole(count):
    return [pl.BlockSpec(memory_space=pltpu.VMEM)] * count


def local_call(kernel, outs, args, scratch=(), flops=0, limit=None):
    many = isinstance(outs, (list, tuple))
    size = sum(a.size * a.dtype.itemsize for a in args)
    return pl.pallas_call(
        kernel,
        out_shape=outs,
        in_specs=whole(len(args)),
        out_specs=whole(len(outs)) if many else whole(1)[0],
        scratch_shapes=list(scratch),
        compiler_params=pltpu.CompilerParams(vmem_limit_bytes=limit or LARGE),
        cost_estimate=pl.CostEstimate(flops=flops, bytes_accessed=size, transcendentals=0),
    )(*args)


def load(ref):
    logs = ref[STATE:, :].astype(F32)
    return ref[0:STATE, :].astype(F32), logs[0:1] + logs[1:2] + logs[2:3]


def quad_order(ordered, refs):
    me = lax.rem(lax.axis_index("sp"), QUAD)
    for bits, ref in enumerate(refs):
        ordered[me ^ bits] = ref[...]


def store(ref, state, log):
    ref[0:STATE, :] = state.astype(BF16)
    high, middle, low = (part.astype(F32) for part in parts_of(log, 3))
    row = lax.broadcasted_iota(jnp.int32, (EXTRA, log.shape[1]), 0)
    logs = jnp.where(row == 0, high, jnp.where(row == 1, middle, jnp.where(row == 2, low, 0.0)))
    ref[STATE:, :] = logs.astype(BF16)


def quad_total_kernel(own, r1, r2, r3, first, sent, state_out, log_out, ordered):
    quad_order(ordered, (own, r1, r2, r3))
    state, log = load(ordered.at[0])
    for place in range(1, QUAD):
        part, part_log = load(ordered.at[place])
        state, log = state * jnp.exp(part_log) + part, log + part_log
    first[...] = state.astype(BF16)
    store(sent, state, log)
    state_out[...] = state
    log_out[...] = log


def jump_kernel(four, before, last, total, total_log, out):
    @pl.when(lax.axis_index("sp") // QUAD == four)
    def _():
        state = before[0:STATE, :].astype(F32)
        if last is not None:
            part, log = load(last)
            state = state * jnp.exp(log) + part
        out[...] = (state * jnp.exp(total_log[...]) + total[...]).astype(BF16)


def choose_kernel(fours, *refs):
    for four, ref in zip(fours, refs, strict=False):

        @pl.when(lax.axis_index("sp") // QUAD == four)
        def _(ref=ref):
            refs[-1][...] = ref[...]


def prefix_kernel(targets, *refs):
    ordered, ends, held, got = refs[-4:]
    quad, outs = refs[-12:-8], refs[-8:-4]
    arrived, pairs = refs[:-13], refs[-13]
    place = lax.axis_index("sp")
    group = place // QUAD
    quad_order(ordered, quad)
    held[...] = jnp.zeros_like(held)
    got[...] = jnp.zeros_like(got)
    for target, ref in zip(targets, arrived, strict=True):

        @pl.when(group == target)
        def _(ref=ref):
            got[...] = ref[0:STATE, :]

    @pl.when(jnp.logical_and(group > max(targets) // 2, lax.rem(group, 2) == 1))
    def _():
        held[...] = pairs[...]

    state, log = load(held)
    state = got[...].astype(F32) * jnp.exp(log) + state
    ends[0] = state.astype(BF16)
    for turn in range(QUAD - 1):
        part, log = load(ordered.at[turn])
        state = state * jnp.exp(log) + part
        ends[turn + 1] = state.astype(BF16)
    me = lax.rem(place, QUAD)
    for bits, out in enumerate(outs):
        out[...] = ends[me ^ bits]


def gate_kernel(gate, cum_all, gate_out, grow_out):
    matrix = spread_matrix(cum_all.shape[0])
    width = 256
    grow = jnp.exp(cum_all[...])
    for start in range(0, gate.shape[1], width):
        lanes = slice(start, start + width)
        gated = silu(gate[:, lanes].astype(F32))
        gate_out[:, lanes] = gated
        grow_out[:, lanes] = gated * spread(grow, matrix[:, lanes])


def inside_kernel(
    x_act, b_act, c_act, edge_x, edge_b, edge_c, cum_all, step_all, gate,
    y_out, c_out, b_all, x_first, padded, turned, entering,
):
    span, _ = x_act.shape
    heads = step_all.shape[0]
    groups = b_act.shape[1] // STATE
    per_group = heads // groups
    matrix = spread_matrix(heads)
    keep = lax.broadcasted_iota(jnp.int32, (BLOCK, BLOCK), 0) >= lax.broadcasted_iota(jnp.int32, (BLOCK, BLOCK), 1)
    left = lax.broadcasted_iota(jnp.int32, (BLOCK, 2 * HEAD_DIM), 1) < HEAD_DIM
    c_out[...] = c_act[...]
    c_out[0:EDGE, :] = edge_c[...]
    b_all[...] = b_act[...]
    b_all[0:EDGE, :] = edge_b[...]
    x_first[...] = x_act[0:BLOCK, :]
    x_first[0:EDGE, :] = edge_x[...]
    padded[...] = jnp.zeros_like(padded)
    before = jnp.zeros((heads, 1), F32)
    for start in range(0, span, BLOCK):
        rows = slice(start, start + BLOCK)
        x_blk = x_first if start == 0 else x_act.at[rows]
        cum = cum_all[:, rows] - before
        step = step_all[:, rows]
        padded[0:heads, :] = cum
        turned[...] = jnp.transpose(padded[...])
        total = cum[:, BLOCK - 1 :]
        before = before + total
        grow = jnp.exp(cum)
        weight = jnp.exp(total - cum) * step
        for group in range(groups):
            lanes = slice(group * STATE, (group + 1) * STATE)
            channels = slice(group * per_group * HEAD_DIM, (group + 1) * per_group * HEAD_DIM)
            b_blk, c_blk = b_all[rows, lanes], c_out[rows, lanes]
            scores = dot(c_blk, b_blk, ((1,), (1,)))
            if start > 0:
                read = dot(c_blk, entering[:, channels].astype(BF16)) * spread(grow, matrix[:, channels])
            for pair in range(per_group // 2):
                first = (group * per_group + 2 * pair) * HEAD_DIM
                results = []
                for head in (group * per_group + 2 * pair, group * per_group + 2 * pair + 1):
                    difference = turned[:, head : head + 1] - cum[head : head + 1, :]
                    decay = jnp.exp(jnp.where(keep, difference, -jnp.inf))
                    mixing = (scores * decay * step[head : head + 1, :]).astype(BF16)
                    results.append(dot(mixing, x_blk[:, first : first + 2 * HEAD_DIM]))
                y = jnp.where(left, results[0], results[1])
                if start > 0:
                    y = y + read[:, 2 * pair * HEAD_DIM : 2 * (pair + 1) * HEAD_DIM]
                y_out[rows, first : first + 2 * HEAD_DIM] = y * gate[rows, first : first + 2 * HEAD_DIM]
            if start + BLOCK < span:
                weighted = (x_blk[:, channels].astype(F32) * spread(weight, matrix[:, channels])).astype(BF16)
                added = dot(b_blk, weighted, ((0,), (0,)))
                if start > 0:
                    grown = spread(jnp.broadcast_to(jnp.exp(total), (heads, BLOCK)), matrix[:, channels], 3)
                    added = entering[:, channels] * grown + added
                entering[:, channels] = added


def output_kernel(own, y_in, grow, c_all, gain, p0, p1, p2, p3, w_out, out, ends, normalized):
    span, inner = y_in.shape
    groups = c_all.shape[1] // STATE
    quarter = inner // QUAD
    half = span // 2
    core = lax.axis_index("tp")
    rows = pl.ds(pl.multiple_of((core if own else 1 - core) * half, 64), half)
    me = own_quarter()
    for bits, ref in enumerate((p0, p1, p2, p3)):
        ends[:, pl.ds(pl.multiple_of((me ^ bits) * quarter, 128), quarter)] = ref[...]
    place = lax.broadcasted_iota(jnp.int32, (quarter, quarter), 0) // HEAD_DIM
    same = place == lax.broadcasted_iota(jnp.int32, (quarter, quarter), 1) // HEAD_DIM
    mean = (same.astype(F32) * (1.0 / HEAD_DIM)).astype(BF16)
    for start in range(0, inner, quarter):
        lanes = slice(start, start + quarter)
        group = start // (inner // groups)
        read = dot(c_all[rows, group * STATE : (group + 1) * STATE], ends[:, lanes])
        gated = y_in[rows, lanes] + read * grow[rows, lanes]
        square = sum(dot(part, mean) for part in parts_of(gated * gated, 2))
        normalized[:, lanes] = (gated * lax.rsqrt(square + EPS) * gain[:, lanes].astype(F32)).astype(BF16)
    width = 512
    for start in range(0, w_out.shape[1], width):
        lanes = slice(start, start + width)
        out[:, lanes] = dot(normalized[...], w_out[:, lanes]).astype(out.dtype)


def sum_kernel(own, other, out):
    out[...] = (own[...] + other[...].astype(F32)).astype(BF16)


def tail_kernel(values, b_in, c_in, out, sems):
    offset, copies = 0, []
    for turn, source in enumerate((b_in, c_in, values)):
        rows, lanes = pl.ds(source.shape[0] - EDGE, EDGE), pl.ds(offset, source.shape[1])
        copies.append(pltpu.make_async_copy(source.at[rows, :], out.at[:, lanes], sems.at[turn]))
        offset += source.shape[1]
    for copy in copies:
        copy.start()
    for copy in copies:
        copy.wait()


def body(
    gate_in, values_in, input_state_in, output_state_in, step_in, conv_x, conv_b, conv_c, dt_bias, decay_rate, log_decay_extra,
    out_gain, w_out,
):
    span, inner = values_in.shape
    shared = input_state_in.shape[1]
    heads = step_in.shape[1]
    places = lax.axis_size("sp")
    quarter = inner // QUAD
    shape = jax.ShapeDtypeStruct
    vmem = pltpu.VMEM

    def move(x, route):
        return lax.ppermute(x, "sp", route)

    def exchange(x, bits, count=places):
        return move(x, [(i, i ^ bits) for i in range(count)])

    tail = pl.pallas_call(
        tail_kernel,
        out_shape=shape((EDGE, inner + 2 * shared), BF16),
        in_specs=[pl.BlockSpec(memory_space=pl.ANY)] * 3,
        out_specs=whole(1)[0],
        scratch_shapes=[pltpu.SemaphoreType.DMA((3,))],
        compiler_params=pltpu.CompilerParams(vmem_limit_bytes=SMALL),
        name="tail",
    )(*(pltpu.with_memory_space_constraint(a, pltpu.HBM) for a in (values_in, input_state_in, output_state_in)))
    halo = move(tail, [(i, i + 1) for i in range(places - 1)])
    args = [
        values_in, input_state_in, output_state_in, step_in.T, log_decay_extra.T, conv_x, conv_b, conv_c,
        dt_bias.reshape(1, heads), decay_rate.reshape(1, heads),
    ]
    outs = [
        shape((span, inner), BF16), shape((span, shared), BF16), shape((span, shared), BF16), shape((heads, span), F32),
        shape((heads, span), F32), shape((STATE, inner), F32), shape((EXTRA, inner), BF16), shape((EDGE, inner), F32),
        shape((EDGE, inner + 2 * shared), BF16),
    ]
    x_act, b_act, c_act, cum, step, state, logs, edge_weight, head = pl.pallas_call(
        local_kernel,
        out_shape=outs,
        in_specs=[pl.BlockSpec(memory_space=pltpu.HBM)] * len(args),
        out_specs=whole(len(outs)),
        scratch_shapes=[vmem((span + 8, 256), F32)] + [vmem(a.shape, a.dtype) for a in args] + [pltpu.SemaphoreType.DMA((len(args),))],
        compiler_params=pltpu.CompilerParams(vmem_limit_bytes=LARGE),
        cost_estimate=pl.CostEstimate(flops=FILL, bytes_accessed=4_000_000, transcendentals=0),
        name="local",
    )(*(pltpu.with_memory_space_constraint(a, pltpu.HBM) for a in args))
    payload = shape((STATE + EXTRA, quarter), BF16)
    edge_x, edge_b, edge_c, *slots = local_call(
        edge_kernel,
        [
            shape((EDGE, inner), BF16), shape((EDGE, shared), BF16), shape((EDGE, shared), BF16), payload, payload, payload, payload,
        ],
        [head, halo, conv_x, conv_b, conv_c, state, logs, edge_weight],
        [vmem((2 * EDGE, inner + 2 * shared), F32), vmem((STATE + EXTRA, inner), BF16)],
        limit=SMALL,
    )

    gate, grow = local_call(gate_kernel, [shape((span, inner), F32)] * 2, [gate_in, cum], flops=FILL)
    y_inside, c_all = local_call(
        inside_kernel,
        [shape((span, inner), F32), shape((span, shared), BF16)],
        [x_act, b_act, c_act, edge_x, edge_b, edge_c, cum, step, gate],
        [
            vmem((span, shared), BF16), vmem((BLOCK, inner), BF16), vmem((BLOCK, BLOCK), F32), vmem((BLOCK, BLOCK), F32),
            vmem((STATE, inner), F32),
        ],
        flops=FILL,
    )

    order = vmem((QUAD, STATE + EXTRA, quarter), BF16)
    arrived = {bits: exchange(slots[bits], bits) for bits in (3, 2, 1)}
    quad = [slots[0], arrived[1], arrived[2], arrived[3]]
    slice_of = shape((STATE, quarter), BF16)
    kept = [shape((STATE, quarter), F32), shape((1, quarter), F32)]
    first, sent, total, log = local_call(quad_total_kernel, [slice_of, payload, *kept], quad, [order], limit=SMALL)
    fours = places // QUAD
    half = fours // 2
    turned = turned_fours(fours)

    def up(x, sources, distance):
        route = []
        for four in sources:
            other = (QUAD - 1) * (turned[four] != turned[four + distance])
            route += [(four * QUAD + i, (four + distance) * QUAD + (i ^ other)) for i in range(QUAD)]
        return move(x, route)

    def jump(four, before, last=None):
        if last is None:
            kernel = lambda *refs: jump_kernel(four, refs[0], None, *refs[1:])
            return local_call(kernel, slice_of, [before, total, log], limit=SMALL)
        return local_call(functools.partial(jump_kernel, four), slice_of, [before, last, total, log], limit=SMALL)

    pairs = up(sent, range(half, fours, 2), 1)
    arrived, targets = [], []

    def send(x, four, distance):
        arrived.append(up(x, (four,), distance))
        targets.append(four + distance)
        return arrived[-1]

    before = send(first, 0, 1)
    for four in range(1, half - 1):
        before = send(jump(four, before), four, 1)
    senders, values = list(range(half - 1, fours - 1, 2)), []
    for four in senders:
        values.append(jump(four, before, pairs if values else None))
        before = send(values[-1], four, 2)
    chosen = local_call(functools.partial(choose_kernel, tuple(senders)), slice_of, values, limit=SMALL)
    side = up(chosen, senders, 1)
    for four in senders:
        arrived.append(side)
        targets.append(four + 1)
    ends = local_call(
        functools.partial(prefix_kernel, tuple(targets)),
        [slice_of] * QUAD,
        [*arrived, pairs, *quad],
        [order, vmem((QUAD, STATE, quarter), BF16), vmem(payload.shape, BF16), vmem(slice_of.shape, BF16)],
        limit=SMALL,
    )
    carried = {bits: exchange(ends[bits], bits) for bits in (3, 2, 1)}

    def projected(own):
        return local_call(
            functools.partial(output_kernel, own),
            shape((span // 2, w_out.shape[1]), F32 if own else BF16),
            [y_inside, grow, c_all, out_gain.reshape(1, inner), ends[0], carried[1], carried[2], carried[3], w_out],
            [vmem((STATE, inner), BF16), vmem((span // 2, inner), BF16)],
            flops=FILL,
        )

    theirs = projected(False)
    other = lax.ppermute(theirs, "tp", [(0, 1), (1, 0)])
    mine = projected(True)
    return local_call(sum_kernel, shape(mine.shape, BF16), [mine, other])


def solution(mesh):
    rows = P(("grp", "sp"), "tp")
    placed = (rows, rows, rows, rows, rows, P(None, "tp"), P(None, "tp"), P(None, "tp"), P("tp"), P("tp"), rows, P("tp"), P("tp", None))
    return jax.shard_map(body, mesh=mesh, in_specs=placed, out_specs=P(("grp", "sp", "tp"), None), check_vma=False)
```
